32 devices in a mesh: sp: 4 (over z), tp: 2 (over y), dp: 4 (over x, core).
Axes of the slice: x: 2, y: 2, z: 4, core: 2. Of those that a mesh axis runs over, the one named last changes fastest.
Arguments:
- latent: bfloat16 [2048, 2048], P(('dp', 'sp', 'tp')), parts along dimension 0, may hold values from -6 to 6
- cond: bfloat16 [8192], P('dp'), parts along dimension 0, may hold values from -6 to 6
- context: bfloat16 [2048, 2048], P(('dp', 'sp')), parts along dimension 0, may hold values from -6 to 6
- context_cond: bfloat16 [2048], replicated, may hold values from -6 to 6
- modulation: bfloat16 [2048, 6144], P(('sp', 'tp')), may hold values from -0.125 to 0.125
- norm_gain: bfloat16 [2048], replicated, may hold values from 0.099609375 to 1.8984375
- w_x: bfloat16 [2048, 1024], P(None, 'tp'), may hold values from -0.125 to 0.125
- w_gate: bfloat16 [2048, 1024], P(None, 'tp'), may hold values from -0.125 to 0.125
- w_b: bfloat16 [2048, 256], P(None, 'tp'), may hold values from -0.125 to 0.125
- w_c: bfloat16 [2048, 256], P(None, 'tp'), may hold values from -0.125 to 0.125
- w_dt: bfloat16 [2, 2048, 16], P(None, None, 'tp'), may hold values from -0.125 to 0.125
- conv_x: bfloat16 [4, 1024], P(None, 'tp'), may hold values from -3 to 3
- conv_b: bfloat16 [4, 256], P(None, 'tp'), may hold values from -3 to 3
- conv_c: bfloat16 [4, 256], P(None, 'tp'), may hold values from -3 to 3
- decay_rate: float32 [2, 16], P(None, 'tp'), may hold values from 0 to 0.04
- decay_extra: float32 [2048, 16], P(('dp', 'sp'), 'tp'), parts along dimension 0, may hold values from -2 to 0
- out_gain: bfloat16 [1024], P('tp'), may hold values from 0.099609375 to 1.8984375
- w_out: bfloat16 [1024, 2048], replicated, may hold values from -0.1875 to 0.1875
Outputs:
- mixed: bfloat16 [2048, 2048], P(('dp', 'sp', 'tp')), parts along dimension 0
The draws below stay inside these ranges and needn't reach their ends.
There are 4 independent parts, one for each index of `dp`. The reference program is written for one: setup_inputs(seed, part) draws one part's arguments, and reference() takes and returns one part's arrays. A program takes and returns all parts, laid end to end along the dimension named above; an argument that names none is the same for every part. Nothing has to cross between parts.
All inputs are finite; a program needn't handle non-finite values.
Results may differ from the reference program's by a relative error of at most 0.007.
Values may be sent and summed in bfloat16 or wider, within the bound.
A program may use at most 64 MiB of HBM per device.

```python
import math
import jax
import jax.numpy as jnp
from jax import lax

D = 2048
MIXER_HEADS = 16
HEAD_DIM = 64
GROUPS = 4
STATE = 64
TAPS = 4
BLOCK = 128
TOK_DEV = 128
CTX = 512
LATENT_TOKENS = 512


def draw_decay_rate(key, part):
    pick_key, fast_key, slow_key = jax.random.split(key, 3)
    fast_share = 0.5
    chosen = jax.random.uniform(pick_key, (2, MIXER_HEADS), jnp.float32) < fast_share
    fast_rate = jnp.exp(jax.random.uniform(fast_key, (2, MIXER_HEADS), jnp.float32, math.log(0.015), math.log(0.04)))
    slow_rate = jnp.exp(jax.random.uniform(slow_key, (2, MIXER_HEADS), jnp.float32, math.log(0.2), 0.0)) / LATENT_TOKENS
    return jnp.where(chosen, fast_rate, slow_rate)


def draw_decay_extra(key, part):
    block_key, head_key, position_random_key, depth_random_key = jax.random.split(key, 4)
    blocks = LATENT_TOKENS // TOK_DEV
    factor = jnp.exp(jax.random.uniform(block_key, (blocks, 1), jnp.float32, 0.0, math.log(8.0)))
    head_scale = jax.random.uniform(head_key, (1, MIXER_HEADS), jnp.float32, 0.5, 1.5)
    steady_portion = jnp.repeat(-(0.2 / LATENT_TOKENS) * factor * head_scale, TOK_DEV, axis=0)
    spike_positions = jax.random.randint(position_random_key, (2,), 0, LATENT_TOKENS)
    spike_depth = jnp.log(jax.random.uniform(depth_random_key, (2, MIXER_HEADS), jnp.float32, 0.5, 0.8))
    spike_rows = (jnp.arange(LATENT_TOKENS)[:, None] == spike_positions[None, :]).astype(jnp.float32)
    return steady_portion + jnp.dot(spike_rows, spike_depth)


def block_scale(rng, extent, pieces, least, largest):
    level, own = 1.0, jax.random.fold_in(rng, 6)
    for position, shards_of in pieces:
        heights = jnp.exp(jax.random.uniform(jax.random.fold_in(own, position), (shards_of,), jnp.float32, least / len(pieces), largest / len(pieces)))
        level = level * jnp.repeat(heights, extent[position] // shards_of).reshape([-1 if axis == position else 1 for axis in range(len(extent))])
    return level


def gaussian(own_key, extent, deviation, reach, cuts=(), held_as=jnp.bfloat16):
    drawn = jax.random.normal(own_key, extent, jnp.float32) * deviation
    if len(cuts) > 0:
        drawn = block_scale(own_key, extent, cuts, -0.22, 0.18) * drawn
    return jnp.clip(drawn, min=-reach, max=reach).astype(held_as)


def setup_inputs(seed: int = 0, part: int = 0) -> dict:
    seeds = jax.random.split(jax.random.key(seed), 19)
    own_keys = jax.random.split(jax.random.fold_in(seeds[18], part), 19)
    return {
        "latent": gaussian(own_keys[0], (LATENT_TOKENS, D), 1.0, 6.0, ((0, 8),)),
        "cond": gaussian(own_keys[1], (D,), 1.0, 6.0),
        "context": gaussian(own_keys[2], (CTX, D), 1.0, 6.0, ((0, 4),)),
        "context_cond": gaussian(seeds[3], (D,), 1.0, 6.0),
        "modulation": gaussian(seeds[4], (D, 3 * D), D ** -0.5, 0.125, ((0, 8),)),
        "norm_gain": jnp.clip(1.0 + 0.18 * jax.random.normal(seeds[5], (D,), jnp.float32), 0.099609375, 1.8984375).astype(jnp.bfloat16),
        "w_x": gaussian(seeds[6], (D, MIXER_HEADS * HEAD_DIM), D ** -0.5, 0.125, ((1, 2),)),
        "w_gate": gaussian(seeds[7], (D, MIXER_HEADS * HEAD_DIM), D ** -0.5, 0.125, ((1, 2),)),
        "w_b": gaussian(seeds[8], (D, GROUPS * STATE), D ** -0.5, 0.125, ((1, 2),)),
        "w_c": gaussian(seeds[9], (D, GROUPS * STATE), D ** -0.5, 0.125, ((1, 2),)),
        "w_dt": gaussian(seeds[10], (2, D, MIXER_HEADS), D ** -0.5, 0.125, ((2, 2),)),
        "conv_x": gaussian(seeds[11], (TAPS, MIXER_HEADS * HEAD_DIM), TAPS ** -0.5, 3.0, ((1, 2),)),
        "conv_b": gaussian(seeds[12], (TAPS, GROUPS * STATE), TAPS ** -0.5, 3.0, ((1, 2),)),
        "conv_c": gaussian(seeds[13], (TAPS, GROUPS * STATE), TAPS ** -0.5, 3.0, ((1, 2),)),
        "decay_rate": draw_decay_rate(jax.random.fold_in(seeds[18], 71), part),
        "decay_extra": draw_decay_extra(jax.random.fold_in(jax.random.fold_in(seeds[18], part), 71), part),
        "out_gain": jnp.clip(1.0 + 0.18 * jax.random.normal(seeds[16], (MIXER_HEADS * HEAD_DIM,), jnp.float32), 0.099609375, 1.8984375).astype(jnp.bfloat16),
        "w_out": gaussian(seeds[17], (MIXER_HEADS * HEAD_DIM, D), (MIXER_HEADS * HEAD_DIM) ** -0.5, 0.1875),
    }


ROW_EPS = 1e-06
GROUP_EPS = 1e-05
HIGHEST = lax.Precision.HIGHEST

def modulated_norm(row_block, norm_gain, shift_row, scale_row):
    values = row_block.astype(jnp.float32)
    normed = values * lax.rsqrt(lax.optimization_barrier(jnp.mean(values * values, axis=-1, keepdims=True)) + ROW_EPS)
    return (normed * norm_gain.astype(jnp.float32) * (1.0 + scale_row) + shift_row).astype(jnp.bfloat16)

def project(row_block, weight):
    return jnp.dot(row_block, weight, preferred_element_type=jnp.float32).astype(jnp.bfloat16)

def conv_padded(padded, conv_taps, length):
    values = padded.astype(jnp.float32)
    summed = jnp.zeros((length, values.shape[1]), jnp.float32)
    for offset in range(conv_taps.shape[0]):
        summed = summed + conv_taps[offset].astype(jnp.float32) * values[offset:offset + length]
    return jax.nn.silu(summed).astype(jnp.bfloat16)

def short_conv(projected, conv_taps):
    padded = jnp.pad(projected, ((2, 1), (0, 0)))
    return conv_padded(padded, conv_taps, projected.shape[0])

def context_states(ctx_xs, ctx_bmat, ctx_dt, decay_rate):
    length = ctx_xs.shape[0]
    groups = ctx_bmat.shape[1] // STATE
    heads_here = ctx_dt.shape[2]
    repeat = heads_here // groups
    values = ctx_xs.astype(jnp.float32).reshape(length, groups, repeat, HEAD_DIM)
    keys_b = ctx_bmat.astype(jnp.float32).reshape(length, groups, STATE)
    log_decay = -decay_rate[:, None, :] * ctx_dt
    running = jnp.cumsum(log_decay, axis=1)
    forward_weight = (jnp.exp(running[0, -1:] - running[0]) * ctx_dt[0]).reshape(length, groups, repeat)
    backward_weight = (jnp.exp(running[1] - log_decay[1]) * ctx_dt[1]).reshape(length, groups, repeat)
    forward_state = jnp.einsum('lgn,lgr,lgrp->grpn', keys_b, forward_weight, values, precision=HIGHEST)
    backward_state = jnp.einsum('lgn,lgr,lgrp->grpn', keys_b, backward_weight, values, precision=HIGHEST)
    return (forward_state, backward_state)

def to_bf16_and_back(values):
    rounded = values.astype(jnp.bfloat16)
    rounded = lax.optimization_barrier(rounded)
    return rounded.astype(jnp.float32)

def block_pass(inputs, step_sizes, log_decay, bmat, cmat, start_state):
    length = inputs.shape[0]
    groups, repeat = (start_state.shape[0], start_state.shape[1])
    block_count = length // BLOCK
    values = inputs.reshape(block_count, BLOCK, groups, repeat, HEAD_DIM)
    steps_blk = step_sizes.reshape(block_count, BLOCK, groups, repeat)
    decays = log_decay.reshape(block_count, BLOCK, groups, repeat)
    keys_b = bmat.reshape(block_count, BLOCK, groups, STATE)
    reads_c = cmat.reshape(block_count, BLOCK, groups, STATE)
    lower_mask = (jnp.arange(BLOCK)[:, None] >= jnp.arange(BLOCK)[None, :])[:, :, None, None]

    def advance(carried, block_data):
        value_blk, step_blk, decay_blk, key_blk, read_blk = block_data
        value_f = value_blk.astype(jnp.float32)
        key_f = key_blk.astype(jnp.float32)
        read_f = read_blk.astype(jnp.float32)
        running = jnp.cumsum(decay_blk, axis=0)
        log_gaps = running[:, None] - running[None, :]
        mixing = jnp.where(lower_mask, jnp.exp(jnp.where(lower_mask, log_gaps, 0.0)), 0.0)
        affinity = jnp.einsum('ign,jgn->ijg', read_f, key_f, precision=HIGHEST)
        weights = to_bf16_and_back(affinity[..., None] * mixing * step_blk[None])
        output = jnp.einsum('ijgr,jgrp->igrp', weights, value_f, precision=HIGHEST)
        output = output + jnp.einsum('ign,grpn,igr->igrp', read_f, carried, jnp.exp(running), precision=HIGHEST)
        to_end = jnp.exp(running[-1:] - running) * step_blk
        state_in = to_bf16_and_back(key_f[:, :, None, :] * to_end[..., None])
        carried = jnp.exp(running[-1])[..., None, None] * carried + jnp.einsum('jgrn,jgrp->grpn', state_in, value_f, precision=HIGHEST)
        return (carried, output)
    final_state, outputs = lax.scan(advance, start_state, (values, steps_blk, decays, keys_b, reads_c))
    return (outputs.reshape(length, groups, repeat, HEAD_DIM), final_state)

def group_norm(combined, out_gain):
    length, groups, repeat, _ = combined.shape
    mean_square = lax.optimization_barrier(jnp.mean(combined * combined, axis=(2, 3), keepdims=True))
    scaled = combined * lax.rsqrt(mean_square + GROUP_EPS) * out_gain.astype(jnp.float32).reshape(groups, repeat, HEAD_DIM)
    return scaled.reshape(length, groups * repeat * HEAD_DIM).astype(jnp.bfloat16)

def reference(latent, cond, context, context_cond, modulation, norm_gain, w_x, w_gate, w_b, w_c, w_dt, conv_x, conv_b, conv_c, decay_rate, decay_extra, out_gain, w_out):
    model_width = latent.shape[1]
    cond_rows = jax.nn.silu(jnp.stack([cond, context_cond]).astype(jnp.float32)).astype(jnp.bfloat16)
    mod_rows = jnp.dot(cond_rows, modulation, preferred_element_type=jnp.float32)
    shift_rows = mod_rows[:, :model_width]
    scale_rows = mod_rows[:, model_width:2 * model_width]
    gate_row = mod_rows[0, 2 * model_width:]
    hidden = modulated_norm(latent, norm_gain, shift_rows[0], scale_rows[0])
    context_hidden = modulated_norm(context, norm_gain, shift_rows[1], scale_rows[1])
    ctx_xs = short_conv(project(context_hidden, w_x), conv_x)
    ctx_bmat = short_conv(project(context_hidden, w_b), conv_b)
    ctx_dt = jnp.stack([jax.nn.softplus(project(context_hidden, w_dt[direction]).astype(jnp.float32)) for direction in range(2)])
    forward_start, backward_start = context_states(ctx_xs, ctx_bmat, ctx_dt, decay_rate)
    latent_xs = short_conv(project(hidden, w_x), conv_x)
    latent_b = short_conv(project(hidden, w_b), conv_b)
    latent_c = short_conv(project(hidden, w_c), conv_c)
    gate_in = project(hidden, w_gate)
    latent_dt = jnp.stack([jax.nn.softplus(project(hidden, w_dt[direction]).astype(jnp.float32)) for direction in range(2)])
    log_decay = -decay_rate[:, None, :] * latent_dt + decay_extra[None]
    y_forward, _ = block_pass(latent_xs, latent_dt[0], log_decay[0], latent_b, latent_c, forward_start)
    y_backward, _ = block_pass(latent_xs[::-1], latent_dt[1][::-1], log_decay[1][::-1], latent_b[::-1], latent_c[::-1], backward_start)
    length, groups, repeat, _ = y_forward.shape
    gate_act = jax.nn.silu(gate_in.astype(jnp.float32)).reshape(length, groups, repeat, HEAD_DIM)
    combined = (y_forward + y_backward[::-1]) * gate_act
    normed = group_norm(combined, out_gain)
    branch = jnp.dot(normed, w_out, preferred_element_type=jnp.float32)
    return (latent.astype(jnp.float32) + gate_row * branch).astype(jnp.bfloat16)
```

```python
import functools

import jax
import jax.numpy as jnp
from jax import lax
from jax.experimental import pallas as pl
from jax.experimental.pallas import tpu as pltpu
from jax.sharding import PartitionSpec as P

HEAD_DIM = 64
STATE = 64
HALO = 16
LANES = 128
ROW_EPS = 1e-06
GROUP_EPS = 1e-05
HIGHEST = lax.Precision.HIGHEST
MESH = pl.DeviceIdType.MESH
F32 = jnp.float32
BF16 = jnp.bfloat16


def silu(v):
    return v / (1.0 + jnp.exp(-v))


def softplus(v):
    return jnp.maximum(v, 0.0) + jnp.log1p(jnp.exp(-jnp.abs(v)))


def dot(a, b):
    return jnp.dot(a, b, preferred_element_type=F32)


def dot_nt(a, b):
    return lax.dot_general(a, b, (((1,), (1,)), ((), ())), preferred_element_type=F32)


def dot_tn(a, b):
    return lax.dot_general(a, b, (((0,), (0,)), ((), ())), preferred_element_type=F32)


def split(v):
    hi = v.astype(BF16)
    return hi, (v - hi.astype(F32)).astype(BF16)


def iota(shape, dim):
    return lax.broadcasted_iota(jnp.int32, shape, dim)


def guarded(always, cond, body):
    if always:
        body()
    else:
        pl.when(cond)(body)


def mixer_kernel(
    n_sp, n_tp, reducers,
    cols_h, latent_h, context_h, modulation_h, gain_h, wx_h, wg_h, wb_h, wc_h, wdt_h,
    cx_h, cb_h, cc_h, dec_h, og_h, wout_h,
    out_h,
    cols, mod_w, gain, wx, wg, wb, wc, wdt, cx, cb, cc, dec, og, wout,
    lat, ctx, lat_prev, lat_next, ctx_prev, ctx_next,
    part, part_rx, mod_full, hid_l, hid_c,
    ctx_msg, lat_msg, lat_rx, y_loc, nrm, nrm_rx, out_v,
    in_sem, halo_send, halo_recv, tok_send, tok_recv,
    rs_send, rs_recv, ag_send, ag_recv,
    cm_send, cm_recv, lm_send, lm_recv, nm_send, nm_recv, out_sem,
):
    s = lax.axis_index("sp")
    t = lax.axis_index("tp")
    n = n_sp * n_tp
    rank = s * n_tp + t
    rows = latent_h.shape[0]
    length = lat.shape[0]
    ctx_len = ctx.shape[0]
    width = lat.shape[1]
    head_cols = wx.shape[1]
    state_cols = wb.shape[1]
    heads = head_cols // HEAD_DIM
    groups = state_cols // STATE
    repeat_cols = head_cols // groups
    chunk = part.shape[2]

    barrier = pltpu.get_barrier_semaphore()

    def group_peer(d):
        other = lax.rem(rank + d, n)
        return {"sp": other // n_tp, "tp": lax.rem(other, n_tp)}

    for d in range(1, n):
        pl.semaphore_signal(barrier, inc=1, device_id=group_peer(d), device_id_type=MESH)

    own_rows = pl.ds(pl.multiple_of(t * rows, 16), rows)
    pairs = [
        (cols_h, cols), (modulation_h, mod_w), (latent_h, lat.at[own_rows]), (context_h, ctx),
        (gain_h, gain), (wx_h, wx), (wb_h, wb), (wdt_h, wdt), (cx_h, cx), (cb_h, cb), (dec_h, dec),
        (wc_h, wc), (cc_h, cc), (wg_h, wg), (og_h, og), (wout_h, wout),
    ]
    loads = [pltpu.make_async_copy(a, b, in_sem.at[i]) for i, (a, b) in enumerate(pairs)]
    for c in loads:
        c.start()
    pl.semaphore_wait(barrier, n - 1)

    sends = []

    def remote(src, dst, ssem, rsem, device):
        return pltpu.make_async_remote_copy(
            src_ref=src, dst_ref=dst, send_sem=ssem, recv_sem=rsem,
            device_id=device, device_id_type=MESH,
        )

    after = lax.rem(s + 1, n_sp)
    before = lax.rem(s + n_sp - 1, n_sp)
    tok = []
    for d in range(1, n_tp):
        c = remote(latent_h, lat.at[own_rows], tok_send.at[d], tok_recv.at[d],
                   {"sp": s, "tp": lax.rem(t + d, n_tp)})
        c.start()
        tok.append(c)
    ctx_halo = [
        remote(context_h.at[pl.ds(ctx_len - HALO, HALO)], ctx_prev, halo_send.at[0],
               halo_recv.at[0], {"sp": after, "tp": t}),
        remote(context_h.at[pl.ds(0, HALO)], ctx_next, halo_send.at[1], halo_recv.at[1],
               {"sp": before, "tp": t}),
    ]
    for c in ctx_halo:
        c.start()
    low = [remote(latent_h.at[pl.ds(rows - HALO, HALO)], lat_prev, halo_send.at[4 + u],
                  halo_recv.at[2], {"sp": after, "tp": u}) for u in range(n_tp)]
    high = [remote(latent_h.at[pl.ds(0, HALO)], lat_next, halo_send.at[4 + n_tp + u],
                   halo_recv.at[3], {"sp": before, "tp": u}) for u in range(n_tp)]

    @pl.when(t == n_tp - 1)
    def _():
        for c in low:
            c.start()

    @pl.when(t == 0)
    def _():
        for c in high:
            c.start()

    loads[0].wait()
    loads[1].wait()
    full = reducers == n
    partial = dot(cols[...], mod_w[...])
    for i in range(reducers):
        part[i] = partial[0:2, i * chunk:(i + 1) * chunk]
    rs = []
    for d in range(1, n):
        other = lax.rem(rank + d, n)
        rs.append(remote(part.at[lax.rem(other, reducers)], part_rx.at[d], rs_send.at[d],
                         rs_recv.at[d], group_peer(d)))
        guarded(full, other < reducers, rs[-1].start)

    for i in (2, 3, 4):
        loads[i].wait()
    ag = [remote(mod_full.at[lax.rem(rank, reducers)], mod_full.at[lax.rem(rank, reducers)],
                 ag_send.at[d], ag_recv.at[d], group_peer(d)) for d in range(1, n)]

    def reduce_chunk():
        total = part[lax.rem(rank, reducers)]
        for d in range(1, n):
            rs[d - 1].wait_recv()
            total = total + part_rx[d]
        mod_full[lax.rem(rank, reducers)] = total
        for c in ag:
            c.start()

    guarded(full, rank < reducers, reduce_chunk)

    def normed_rows(halo_prev, halo_next, body):
        edge = jnp.where(
            iota((HALO, width), 0) == 0,
            halo_next[...].astype(F32),
            halo_prev[...].astype(F32),
        )
        values = jnp.concatenate([edge, body[...].astype(F32)], axis=0)
        return values, lax.rsqrt(jnp.mean(values * values, axis=-1, keepdims=True) + ROW_EPS)

    for c in ctx_halo:
        c.wait_recv()
    ctx_vals, ctx_rs = normed_rows(ctx_prev, ctx_next, ctx)
    gain_row = gain[...].astype(F32)

    for d in range(1, n):
        source = lax.rem(rank + n - d, n)
        guarded(full, source < reducers, ag[d - 1].wait_recv)
    mod_rows = jnp.concatenate([mod_full[i] for i in range(reducers)], axis=1)
    shift = mod_rows[:, :width]
    scale = mod_rows[:, width:2 * width]
    gate_row = mod_rows[0:1, 2 * width:]

    def conv(z, taps_ref):
        total_rows = z.shape[0]
        has_prev = jnp.where(s > 0, 1, 0)
        has_next = jnp.where(s < n_sp - 1, 1, 0)
        r = iota(z.shape, 0)
        keep = jnp.where(r == 0, has_next, jnp.where(r < HALO, has_prev, 1))
        z = jnp.where(keep > 0, z, 0.0)
        taps = taps_ref[...].astype(F32)
        u = (
            taps[0:1] * pltpu.roll(z, 2, 0)
            + taps[1:2] * pltpu.roll(z, 1, 0)
            + taps[2:3] * z
            + taps[3:4] * pltpu.roll(z, total_rows - 1, 0)
        )
        return silu(u[HALO:])

    lane_row = iota((1, LANES), 1)
    expander = (
        iota((LANES, 2 * head_cols), 0) == iota((LANES, 2 * head_cols), 1) // HEAD_DIM
    ).astype(F32).astype(BF16)

    def expand(v):
        hi, lo = split(v)
        return dot(hi, expander) + dot(lo, expander)

    def decay_run(log_decay):
        size = log_decay.shape[0]
        i = iota((size, size), 0)
        j = iota((size, size), 1)
        pre = jnp.dot((j <= i).astype(F32), log_decay, precision=HIGHEST,
                      preferred_element_type=F32)
        total = pre[size - 1:size]
        suf = total - pre + log_decay
        return jnp.where(lane_row < heads, pre, suf), total

    def summarize(msg, xs, bm, dt, run, total):
        weight = expand(jnp.exp(total - run) * dt)
        thi, tlo = split(jnp.broadcast_to(total, (16, LANES)))
        tail_hi = dot(thi, expander)
        tail_lo = dot(tlo, expander)
        row = iota((16, repeat_cols), 0)
        for d in range(2):
            base = d * head_cols
            state = dot_tn(bm, (xs * weight[:, base:base + head_cols]).astype(BF16))
            tail = jnp.zeros((16, repeat_cols), F32)
            for g in range(groups):
                lo_c = base + g * repeat_cols
                msg[d, g * STATE:(g + 1) * STATE, :] = state[
                    g * STATE:(g + 1) * STATE, g * repeat_cols:(g + 1) * repeat_cols
                ].astype(BF16)
                tail = jnp.where(row == g, tail_hi[:, lo_c:lo_c + repeat_cols], tail)
                tail = jnp.where(row == groups + g, tail_lo[:, lo_c:lo_c + repeat_cols], tail)
            msg[d, groups * STATE:, :] = tail.astype(BF16)

    hid_c[...] = (
        ctx_vals * ctx_rs * gain_row * (1.0 + scale[1:2]) + shift[1:2]
    ).astype(BF16)
    for i in (5, 6, 7, 8, 9, 10):
        loads[i].wait()
    rate_row = dec[length:length + 1, :]
    ctx_x = conv(dot(hid_c[...], wx[...]), cx)
    ctx_b = conv(dot(hid_c[...], wb[...]), cb).astype(BF16)
    ctx_dt = softplus(dot(hid_c[HALO:, :], wdt[...]))
    ctx_run, ctx_total = decay_run(rate_row * ctx_dt)
    summarize(ctx_msg.at[0], ctx_x, ctx_b, ctx_dt, ctx_run, ctx_total)
    cm = []
    for d in range(1, n_sp):
        c = remote(ctx_msg.at[0], ctx_msg.at[d], cm_send.at[d], cm_recv.at[d],
                   {"sp": lax.rem(s + d, n_sp), "tp": t})
        c.start()
        cm.append(c)

    for c in tok:
        c.wait_recv()
    low[0].wait_recv()
    high[0].wait_recv()
    lat_vals, lat_rs = normed_rows(lat_prev, lat_next, lat)
    hid_l[...] = (
        lat_vals * lat_rs * gain_row * (1.0 + scale[0:1]) + shift[0:1]
    ).astype(BF16)
    lat_x = conv(dot(hid_l[...], wx[...]), cx)
    lat_b = conv(dot(hid_l[...], wb[...]), cb).astype(BF16)
    dt = softplus(dot(hid_l[HALO:, :], wdt[...]))
    run, total = decay_run(rate_row * dt + dec[0:length, :])
    summarize(lat_msg, lat_x, lat_b, dt, run, total)
    lm = []
    for d in range(1, n_sp):
        c = remote(lat_msg.at[(s + d) // n_sp], lat_rx.at[d], lm_send.at[d], lm_recv.at[d],
                   {"sp": lax.rem(s + d, n_sp), "tp": t})
        c.start()
        lm.append(c)

    loads[11].wait()
    loads[12].wait()
    lat_c = conv(dot(hid_l[...], wc[...]), cc).astype(BF16)
    run_t = jnp.transpose(run)
    dt_t = jnp.transpose(dt)
    i_pos = iota((length, length), 0)
    j_pos = iota((length, length), 1)
    lat_xb = lat_x.astype(BF16)
    state_lane = iota((length, state_cols), 1) // STATE
    pair_lane = iota((length, LANES), 1)
    zero_b = jnp.zeros((), BF16)
    per_group = heads // groups
    affinity = [
        dot_nt(jnp.where(state_lane == g, lat_c, zero_b), lat_b) for g in range(groups)
    ]

    def block_weights(h):
        ahead = heads + h
        gap = jnp.where(
            j_pos <= i_pos,
            run[:, h:h + 1] - run_t[h:h + 1, :],
            run[:, ahead:ahead + 1] - run_t[ahead:ahead + 1, :],
        )
        step = jnp.where(j_pos <= i_pos, dt_t[h:h + 1, :], 0.0) + jnp.where(
            j_pos >= i_pos, dt_t[ahead:ahead + 1, :], 0.0
        )
        return (affinity[h // per_group] * jnp.exp(gap) * step).astype(BF16)

    for q in range(heads // 2):
        both = lat_xb[:, q * LANES:(q + 1) * LANES]
        y_loc[:, q * LANES:(q + 1) * LANES] = dot(
            jnp.concatenate([block_weights(2 * q), block_weights(2 * q + 1)], axis=1),
            jnp.concatenate(
                [
                    jnp.where(pair_lane < HEAD_DIM, both, zero_b),
                    jnp.where(pair_lane >= HEAD_DIM, both, zero_b),
                ],
                axis=0,
            ),
        )
    reach = expand(jnp.exp(run))
    loads[13].wait()
    loads[14].wait()
    gate_act = silu(dot(hid_l[HALO:, :], wg[...]))

    def totals(tail):
        rows16 = tail.astype(F32)
        return [rows16[g:g + 1] + rows16[groups + g:groups + g + 1] for g in range(groups)]

    srows = [pl.ds(g * STATE, STATE) for g in range(groups)]
    trows = pl.ds(groups * STATE, 16)
    for c in cm:
        c.wait_recv()
    start = []
    for d in range(2):
        acc = [jnp.zeros((1, repeat_cols), F32) for _ in range(groups)]
        state = [jnp.zeros((STATE, repeat_cols), F32) for _ in range(groups)]
        for k in range(n_sp):
            place = n_sp - 1 - k if d == 0 else k
            slot = lax.rem(s + n_sp - place, n_sp)
            tot = totals(ctx_msg[slot, d, trows, :])
            for g in range(groups):
                state[g] = state[g] + jnp.exp(acc[g]) * ctx_msg[slot, d, srows[g], :].astype(F32)
                acc[g] = acc[g] + tot[g]
        start.append(state)
    for c in lm:
        c.wait_recv()
    mixed_y = y_loc[...]
    for d in range(2):
        acc = [jnp.zeros((1, repeat_cols), F32) for _ in range(groups)]
        state = [jnp.zeros((STATE, repeat_cols), F32) for _ in range(groups)]
        for e in range(1, n_sp):
            slot = e if d == 0 else n_sp - e
            valid = (s >= e) if d == 0 else (s + e < n_sp)
            live = jnp.where(valid, 1.0, 0.0)
            tot = totals(lat_rx[slot, trows, :])
            for g in range(groups):
                state[g] = state[g] + live * (
                    jnp.exp(acc[g]) * lat_rx[slot, srows[g], :].astype(F32)
                )
                acc[g] = acc[g] + live * tot[g]
        blocks = []
        for g in range(groups):
            entry = (state[g] + jnp.exp(acc[g]) * start[d][g]).astype(BF16)
            pieces = [
                entry if k == g else jnp.zeros((STATE, repeat_cols), BF16) for k in range(groups)
            ]
            blocks.append(jnp.concatenate(pieces, axis=1) if groups > 1 else entry)
        entry_all = jnp.concatenate(blocks, axis=0) if groups > 1 else blocks[0]
        mixed_y = mixed_y + reach[:, d * head_cols:(d + 1) * head_cols] * dot(lat_c, entry_all)
    gated = mixed_y * gate_act
    og_row = og[...].astype(F32)
    for g in range(groups):
        part_g = gated[:, g * repeat_cols:(g + 1) * repeat_cols]
        ms = jnp.mean(part_g * part_g, axis=-1, keepdims=True)
        nrm[:, g * repeat_cols:(g + 1) * repeat_cols] = (
            part_g * lax.rsqrt(ms + GROUP_EPS) * og_row[:, g * repeat_cols:(g + 1) * repeat_cols]
        ).astype(BF16)

    nm = []
    for d in range(1, n_tp):
        u = lax.rem(t + d, n_tp)
        c = remote(nrm.at[pl.ds(pl.multiple_of(u * rows, 16), rows)], nrm_rx.at[d],
                   nm_send.at[d], nm_recv.at[d], {"sp": s, "tp": u})
        c.start()
        nm.append(c)
    loads[15].wait()

    def out_rows(u):
        return wout[pl.ds(pl.multiple_of(u * head_cols, 16), head_cols), :]

    branch = dot(nrm[own_rows, :], out_rows(t))
    for d in range(1, n_tp):
        nm[d - 1].wait_recv()
        branch = branch + dot(nrm_rx[d], out_rows(lax.rem(t + n_tp - d, n_tp)))
    out_v[...] = (lat[own_rows, :].astype(F32) + gate_row * branch).astype(BF16)
    final = pltpu.make_async_copy(out_v, out_h, out_sem)
    final.start()

    for c in tok + ctx_halo + cm + lm + nm:
        c.wait_send()

    @pl.when(t == n_tp - 1)
    def _():
        for c in low:
            c.wait_send()

    @pl.when(t == 0)
    def _():
        for c in high:
            c.wait_send()

    for d in range(1, n):
        other = lax.rem(rank + d, n)
        guarded(full, other < reducers, rs[d - 1].wait_send)

    def ag_done():
        for c in ag:
            c.wait_send()

    guarded(full, rank < reducers, ag_done)
    final.wait()


def local(
    latent, cond, context, context_cond, modulation, norm_gain, w_x, w_gate, w_b, w_c, w_dt,
    conv_x, conv_b, conv_c, decay_rate, decay_extra, out_gain, w_out,
):
    n_sp = lax.axis_size("sp")
    n_tp = lax.axis_size("tp")
    n = n_sp * n_tp
    rows, width = latent.shape
    length = decay_extra.shape[0]
    ctx_len = context.shape[0]
    share = modulation.shape[0]
    mod_cols = modulation.shape[1]
    head_cols = w_x.shape[1]
    state_cols = w_b.shape[1]
    heads = w_dt.shape[2]
    groups = state_cols // STATE
    repeat_cols = head_cols // groups
    reducers = max(m for m in range(1, n + 1) if mod_cols % (LANES * m) == 0)
    chunk = mod_cols // reducers

    cond_rows = silu(jnp.stack([cond, context_cond]).astype(F32)).astype(BF16)
    own_cols = lax.dynamic_slice_in_dim(
        cond_rows, lax.axis_index(("sp", "tp")) * share, share, 1
    )
    cols = jnp.pad(own_cols, ((0, 14), (0, 0)))
    wdt = jnp.pad(
        jnp.concatenate([w_dt[0], w_dt[1]], axis=1), ((0, 0), (0, LANES - 2 * heads))
    )
    dec = jnp.pad(
        jnp.concatenate(
            [
                jnp.concatenate([decay_extra, decay_extra], axis=1),
                jnp.broadcast_to(-decay_rate.reshape(1, 2 * heads), (8, 2 * heads)),
            ],
            axis=0,
        ),
        ((0, 0), (0, LANES - 2 * heads)),
    )
    args = (
        cols, latent, context, modulation, norm_gain.reshape(1, width), w_x, w_gate, w_b, w_c,
        wdt, conv_x, conv_b, conv_c, dec, out_gain.reshape(1, head_cols), w_out,
    )
    V = pltpu.VMEM
    D = pltpu.SemaphoreType.DMA
    held = [args[i] for i in (0, 3, 4, 5, 6, 7, 8, 9, 10, 11, 12, 13, 14, 15)]
    msg = (groups * STATE + 16, repeat_cols)
    scratch = [V(a.shape, a.dtype) for a in held] + [
        V((length, width), BF16),
        V((ctx_len, width), BF16),
        V((HALO, width), BF16),
        V((HALO, width), BF16),
        V((HALO, width), BF16),
        V((HALO, width), BF16),
        V((reducers, 2, chunk), F32),
        V((n, 2, chunk), F32),
        V((reducers, 2, chunk), F32),
        V((length + HALO, width), BF16),
        V((ctx_len + HALO, width), BF16),
        V((n_sp, 2) + msg, BF16),
        V((2,) + msg, BF16),
        V((n_sp,) + msg, BF16),
        V((length, head_cols), F32),
        V((length, head_cols), BF16),
        V((n_tp, rows, head_cols), BF16),
        V((rows, width), BF16),
        D((len(args),)),
        D((4 + 2 * n_tp,)),
        D((4,)),
        D((n_tp,)), D((n_tp,)),
        D((n,)), D((n,)), D((n,)), D((n,)),
        D((n_sp,)), D((n_sp,)), D((n_sp,)), D((n_sp,)),
        D((n_tp,)), D((n_tp,)),
        D,
    ]
    return pl.pallas_call(
        functools.partial(mixer_kernel, n_sp, n_tp, reducers),
        out_shape=jax.ShapeDtypeStruct((rows, width), BF16),
        in_specs=[pl.BlockSpec(memory_space=pl.ANY)] * len(args),
        out_specs=pl.BlockSpec(memory_space=pl.ANY),
        scratch_shapes=scratch,
        compiler_params=pltpu.CompilerParams(
            collective_id=0, has_side_effects=True, vmem_limit_bytes=60 * 1024 * 1024
        ),
    )(*args)


def solution(mesh):
    in_specs = (
        P(("dp", "sp", "tp"), None),
        P("dp"),
        P(("dp", "sp"), None),
        P(),
        P(("sp", "tp"), None),
        P(),
        P(None, "tp"),
        P(None, "tp"),
        P(None, "tp"),
        P(None, "tp"),
        P(None, None, "tp"),
        P(None, "tp"),
        P(None, "tp"),
        P(None, "tp"),
        P(None, "tp"),
        P(("dp", "sp"), "tp"),
        P("tp"),
        P(),
    )
    out_specs = P(("dp", "sp", "tp"), None)
    return jax.shard_map(local, mesh=mesh, in_specs=in_specs, out_specs=out_specs, check_vma=False)
```

```python
import functools

import jax
import jax.numpy as jnp
from jax import lax
from jax.experimental import pallas as pl
from jax.experimental.pallas import tpu as pltpu
from jax.sharding import PartitionSpec as P

HEAD_DIM = 64
STATE = 64
HALO = 16
LANES = 128
ROW_EPS = 1e-06
GROUP_EPS = 1e-05
HIGHEST = lax.Precision.HIGHEST
MESH = pl.DeviceIdType.MESH
F32 = jnp.float32
BF16 = jnp.bfloat16


def silu(v):
    return v / (1.0 + jnp.exp(-v))


def softplus(v):
    return jnp.maximum(v, 0.0) + jnp.log1p(jnp.exp(-jnp.abs(v)))


def dot(a, b):
    return jnp.dot(a, b, preferred_element_type=F32)


def dot_nt(a, b):
    return lax.dot_general(a, b, (((1,), (1,)), ((), ())), preferred_element_type=F32)


def dot_tn(a, b):
    return lax.dot_general(a, b, (((0,), (0,)), ((), ())), preferred_element_type=F32)


def split(v):
    hi = v.astype(BF16)
    return hi, (v - hi.astype(F32)).astype(BF16)


def iota(shape, dim):
    return lax.broadcasted_iota(jnp.int32, shape, dim)


def flat_row(tiled):
    return jnp.concatenate([tiled[i:i + 1] for i in range(tiled.shape[0])], axis=1)


def own_cond(rows_ref, k, rank, share):
    if share % LANES == 0:
        count = share // LANES
        return jnp.concatenate(
            [rows_ref[k, pl.ds(rank * count + i, 1), :] for i in range(count)], axis=1
        )
    per = LANES // share
    row = jnp.broadcast_to(rows_ref[k, pl.ds(rank // per, 1), :], (8, LANES))
    moved = pltpu.roll(row, lax.rem(LANES - lax.rem(rank, per) * share, LANES), 1)
    return moved[0:1, :share]


def guarded(always, cond, body):
    if always:
        body()
    else:
        pl.when(cond)(body)


def mixer_kernel(
    n_sp, n_tp, reducers,
    cond_h, latent_h, context_h, modulation_h, gain_h, wx_h, wg_h, wb_h, wc_h, wdt_h,
    cx_h, cb_h, cc_h, extra_h, og_h, wout_h, ccond_h, rate_h,
    out_h,
    cond, mod_w, gain, wx, wg, wb, wc, wdt, cx, cb, cc, extra, og, wout, ccond, rate,
    cond_rows, wdt_all,
    lat, ctx, lat_prev, lat_next, ctx_prev, ctx_next,
    part, part_rx, mod_full, hid_l, hid_c,
    ctx_msg, lat_msg, lat_rx, y_loc, nrm, nrm_rx, out_v,
    in_sem, halo_send, halo_recv, tok_send, tok_recv,
    rs_send, rs_recv, ag_send, ag_recv,
    cm_send, cm_recv, lm_send, lm_recv, nm_send, nm_recv, out_sem,
):
    s = lax.axis_index("sp")
    t = lax.axis_index("tp")
    n = n_sp * n_tp
    rank = s * n_tp + t
    rows = latent_h.shape[0]
    length = lat.shape[0]
    ctx_len = ctx.shape[0]
    width = lat.shape[1]
    head_cols = wx.shape[1]
    state_cols = wb.shape[1]
    heads = head_cols // HEAD_DIM
    groups = state_cols // STATE
    repeat_cols = head_cols // groups
    chunk = part.shape[2]

    barrier = pltpu.get_barrier_semaphore()

    def group_peer(d):
        other = lax.rem(rank + d, n)
        return {"sp": other // n_tp, "tp": lax.rem(other, n_tp)}

    for d in range(1, n):
        pl.semaphore_signal(barrier, inc=1, device_id=group_peer(d), device_id_type=MESH)

    own_rows = pl.ds(pl.multiple_of(t * rows, 16), rows)
    pairs = [
        (cond_h, cond), (modulation_h, mod_w), (latent_h, lat.at[own_rows]), (context_h, ctx),
        (gain_h, gain), (wx_h, wx), (wb_h, wb), (wdt_h, wdt), (cx_h, cx), (cb_h, cb),
        (extra_h, extra), (wc_h, wc), (cc_h, cc), (wg_h, wg), (og_h, og), (wout_h, wout),
        (ccond_h, ccond), (rate_h, rate),
    ]
    loads = [pltpu.make_async_copy(a, b, in_sem.at[i]) for i, (a, b) in enumerate(pairs)]
    for c in loads:
        c.start()
    pl.semaphore_wait(barrier, n - 1)

    sends = []

    def remote(src, dst, ssem, rsem, device):
        return pltpu.make_async_remote_copy(
            src_ref=src, dst_ref=dst, send_sem=ssem, recv_sem=rsem,
            device_id=device, device_id_type=MESH,
        )

    after = lax.rem(s + 1, n_sp)
    before = lax.rem(s + n_sp - 1, n_sp)
    tok = []
    for d in range(1, n_tp):
        c = remote(latent_h, lat.at[own_rows], tok_send.at[d], tok_recv.at[d],
                   {"sp": s, "tp": lax.rem(t + d, n_tp)})
        c.start()
        tok.append(c)
    ctx_halo = [
        remote(context_h.at[pl.ds(ctx_len - HALO, HALO)], ctx_prev, halo_send.at[0],
               halo_recv.at[0], {"sp": after, "tp": t}),
        remote(context_h.at[pl.ds(0, HALO)], ctx_next, halo_send.at[1], halo_recv.at[1],
               {"sp": before, "tp": t}),
    ]
    for c in ctx_halo:
        c.start()
    low = [remote(latent_h.at[pl.ds(rows - HALO, HALO)], lat_prev, halo_send.at[4 + u],
                  halo_recv.at[2], {"sp": after, "tp": u}) for u in range(n_tp)]
    high = [remote(latent_h.at[pl.ds(0, HALO)], lat_next, halo_send.at[4 + n_tp + u],
                   halo_recv.at[3], {"sp": before, "tp": u}) for u in range(n_tp)]

    @pl.when(t == n_tp - 1)
    def _():
        for c in low:
            c.start()

    @pl.when(t == 0)
    def _():
        for c in high:
            c.start()

    loads[0].wait()
    loads[16].wait()
    cond_rows[0] = silu(cond[...].astype(F32))
    cond_rows[1] = silu(ccond[...].astype(F32))
    own = [own_cond(cond_rows, k, rank, mod_w.shape[0]) for k in range(2)]
    pick = iota((16, mod_w.shape[0]), 0)
    cols = jnp.where(pick == 0, own[0], jnp.where(pick == 1, own[1], 0.0)).astype(BF16)
    loads[1].wait()
    full = reducers == n
    partial = dot(cols, mod_w[...])
    for i in range(reducers):
        part[i] = partial[0:2, i * chunk:(i + 1) * chunk]
    rs = []
    for d in range(1, n):
        other = lax.rem(rank + d, n)
        rs.append(remote(part.at[lax.rem(other, reducers)], part_rx.at[d], rs_send.at[d],
                         rs_recv.at[d], group_peer(d)))
        guarded(full, other < reducers, rs[-1].start)

    for i in (2, 3, 4):
        loads[i].wait()
    ag = [remote(mod_full.at[lax.rem(rank, reducers)], mod_full.at[lax.rem(rank, reducers)],
                 ag_send.at[d], ag_recv.at[d], group_peer(d)) for d in range(1, n)]

    def reduce_chunk():
        total = part[lax.rem(rank, reducers)]
        for d in range(1, n):
            rs[d - 1].wait_recv()
            total = total + part_rx[d]
        mod_full[lax.rem(rank, reducers)] = total
        for c in ag:
            c.start()

    guarded(full, rank < reducers, reduce_chunk)

    def normed_rows(halo_prev, halo_next, body):
        edge = jnp.where(
            iota((HALO, width), 0) == 0,
            halo_next[...].astype(F32),
            halo_prev[...].astype(F32),
        )
        values = jnp.concatenate([edge, body[...].astype(F32)], axis=0)
        return values, lax.rsqrt(jnp.mean(values * values, axis=-1, keepdims=True) + ROW_EPS)

    for c in ctx_halo:
        c.wait_recv()
    ctx_vals, ctx_rs = normed_rows(ctx_prev, ctx_next, ctx)
    gain_row = flat_row(gain[...].astype(F32))
    for i in (7, 10, 17):
        loads[i].wait()
    spare = LANES - 2 * heads
    wdt_all[...] = jnp.concatenate(
        [wdt[0].astype(F32), wdt[1].astype(F32), jnp.zeros((spare, width), F32)], axis=0
    ).astype(BF16)
    extra_all = jnp.transpose(
        jnp.concatenate([extra[...], extra[...], jnp.zeros((spare, length), F32)], axis=0)
    )
    rate_row = -jnp.concatenate([rate[0:1, :], rate[1:2, :], jnp.zeros((1, spare), F32)], axis=1)

    for d in range(1, n):
        source = lax.rem(rank + n - d, n)
        guarded(full, source < reducers, ag[d - 1].wait_recv)
    mod_rows = jnp.concatenate([mod_full[i] for i in range(reducers)], axis=1)
    shift = mod_rows[:, :width]
    scale = mod_rows[:, width:2 * width]
    gate_row = mod_rows[0:1, 2 * width:]

    def conv(z, taps_ref):
        total_rows = z.shape[0]
        has_prev = jnp.where(s > 0, 1, 0)
        has_next = jnp.where(s < n_sp - 1, 1, 0)
        r = iota(z.shape, 0)
        keep = jnp.where(r == 0, has_next, jnp.where(r < HALO, has_prev, 1))
        z = jnp.where(keep > 0, z, 0.0)
        taps = taps_ref[...].astype(F32)
        u = (
            taps[0:1] * pltpu.roll(z, 2, 0)
            + taps[1:2] * pltpu.roll(z, 1, 0)
            + taps[2:3] * z
            + taps[3:4] * pltpu.roll(z, total_rows - 1, 0)
        )
        return silu(u[HALO:])

    lane_row = iota((1, LANES), 1)
    expander = (
        iota((LANES, 2 * head_cols), 0) == iota((LANES, 2 * head_cols), 1) // HEAD_DIM
    ).astype(F32).astype(BF16)

    def expand(v):
        hi, lo = split(v)
        return dot(hi, expander) + dot(lo, expander)

    def decay_run(log_decay):
        size = log_decay.shape[0]
        i = iota((size, size), 0)
        j = iota((size, size), 1)
        pre = jnp.dot((j <= i).astype(F32), log_decay, precision=HIGHEST,
                      preferred_element_type=F32)
        total = pre[size - 1:size]
        suf = total - pre + log_decay
        return jnp.where(lane_row < heads, pre, suf), total

    def summarize(msg, xs, bm, dt, run, total):
        weight = expand(jnp.exp(total - run) * dt)
        thi, tlo = split(jnp.broadcast_to(total, (16, LANES)))
        tail_hi = dot(thi, expander)
        tail_lo = dot(tlo, expander)
        row = iota((16, repeat_cols), 0)
        for d in range(2):
            base = d * head_cols
            state = dot_tn(bm, (xs * weight[:, base:base + head_cols]).astype(BF16))
            tail = jnp.zeros((16, repeat_cols), F32)
            for g in range(groups):
                lo_c = base + g * repeat_cols
                msg[d, g * STATE:(g + 1) * STATE, :] = state[
                    g * STATE:(g + 1) * STATE, g * repeat_cols:(g + 1) * repeat_cols
                ].astype(BF16)
                tail = jnp.where(row == g, tail_hi[:, lo_c:lo_c + repeat_cols], tail)
                tail = jnp.where(row == groups + g, tail_lo[:, lo_c:lo_c + repeat_cols], tail)
            msg[d, groups * STATE:, :] = tail.astype(BF16)

    hid_c[...] = (
        ctx_vals * ctx_rs * gain_row * (1.0 + scale[1:2]) + shift[1:2]
    ).astype(BF16)
    for i in (5, 6, 8, 9):
        loads[i].wait()
    ctx_x = conv(dot(hid_c[...], wx[...]), cx)
    ctx_b = conv(dot(hid_c[...], wb[...]), cb).astype(BF16)
    ctx_dt = softplus(dot_nt(hid_c[HALO:, :], wdt_all[...]))
    ctx_run, ctx_total = decay_run(rate_row * ctx_dt)
    summarize(ctx_msg.at[0], ctx_x, ctx_b, ctx_dt, ctx_run, ctx_total)
    cm = []
    for d in range(1, n_sp):
        c = remote(ctx_msg.at[0], ctx_msg.at[d], cm_send.at[d], cm_recv.at[d],
                   {"sp": lax.rem(s + d, n_sp), "tp": t})
        c.start()
        cm.append(c)

    for c in tok:
        c.wait_recv()
    low[0].wait_recv()
    high[0].wait_recv()
    lat_vals, lat_rs = normed_rows(lat_prev, lat_next, lat)
    hid_l[...] = (
        lat_vals * lat_rs * gain_row * (1.0 + scale[0:1]) + shift[0:1]
    ).astype(BF16)
    lat_x = conv(dot(hid_l[...], wx[...]), cx)
    lat_b = conv(dot(hid_l[...], wb[...]), cb).astype(BF16)
    dt = softplus(dot_nt(hid_l[HALO:, :], wdt_all[...]))
    run, total = decay_run(rate_row * dt + extra_all)
    summarize(lat_msg, lat_x, lat_b, dt, run, total)
    lm = []
    for d in range(1, n_sp):
        c = remote(lat_msg.at[(s + d) // n_sp], lat_rx.at[d], lm_send.at[d], lm_recv.at[d],
                   {"sp": lax.rem(s + d, n_sp), "tp": t})
        c.start()
        lm.append(c)

    loads[11].wait()
    loads[12].wait()
    lat_c = conv(dot(hid_l[...], wc[...]), cc).astype(BF16)
    run_t = jnp.transpose(run)
    dt_t = jnp.transpose(dt)
    i_pos = iota((length, length), 0)
    j_pos = iota((length, length), 1)
    lat_xb = lat_x.astype(BF16)
    state_lane = iota((length, state_cols), 1) // STATE
    pair_lane = iota((length, LANES), 1)
    zero_b = jnp.zeros((), BF16)
    per_group = heads // groups
    affinity = [
        dot_nt(jnp.where(state_lane == g, lat_c, zero_b), lat_b) for g in range(groups)
    ]

    def block_weights(h):
        ahead = heads + h
        gap = jnp.where(
            j_pos <= i_pos,
            run[:, h:h + 1] - run_t[h:h + 1, :],
            run[:, ahead:ahead + 1] - run_t[ahead:ahead + 1, :],
        )
        step = jnp.where(j_pos <= i_pos, dt_t[h:h + 1, :], 0.0) + jnp.where(
            j_pos >= i_pos, dt_t[ahead:ahead + 1, :], 0.0
        )
        return (affinity[h // per_group] * jnp.exp(gap) * step).astype(BF16)

    for q in range(heads // 2):
        both = lat_xb[:, q * LANES:(q + 1) * LANES]
        y_loc[:, q * LANES:(q + 1) * LANES] = dot(
            jnp.concatenate([block_weights(2 * q), block_weights(2 * q + 1)], axis=1),
            jnp.concatenate(
                [
                    jnp.where(pair_lane < HEAD_DIM, both, zero_b),
                    jnp.where(pair_lane >= HEAD_DIM, both, zero_b),
                ],
                axis=0,
            ),
        )
    reach = expand(jnp.exp(run))
    loads[13].wait()
    loads[14].wait()
    gate_act = silu(dot(hid_l[HALO:, :], wg[...]))

    def totals(tail):
        rows16 = tail.astype(F32)
        return [rows16[g:g + 1] + rows16[groups + g:groups + g + 1] for g in range(groups)]

    srows = [pl.ds(g * STATE, STATE) for g in range(groups)]
    trows = pl.ds(groups * STATE, 16)
    for c in cm:
        c.wait_recv()
    start = []
    for d in range(2):
        acc = [jnp.zeros((1, repeat_cols), F32) for _ in range(groups)]
        state = [jnp.zeros((STATE, repeat_cols), F32) for _ in range(groups)]
        for k in range(n_sp):
            place = n_sp - 1 - k if d == 0 else k
            slot = lax.rem(s + n_sp - place, n_sp)
            tot = totals(ctx_msg[slot, d, trows, :])
            for g in range(groups):
                state[g] = state[g] + jnp.exp(acc[g]) * ctx_msg[slot, d, srows[g], :].astype(F32)
                acc[g] = acc[g] + tot[g]
        start.append(state)
    for c in lm:
        c.wait_recv()
    mixed_y = y_loc[...]
    for d in range(2):
        acc = [jnp.zeros((1, repeat_cols), F32) for _ in range(groups)]
        state = [jnp.zeros((STATE, repeat_cols), F32) for _ in range(groups)]
        for e in range(1, n_sp):
            slot = e if d == 0 else n_sp - e
            valid = (s >= e) if d == 0 else (s + e < n_sp)
            live = jnp.where(valid, 1.0, 0.0)
            tot = totals(lat_rx[slot, trows, :])
            for g in range(groups):
                state[g] = state[g] + live * (
                    jnp.exp(acc[g]) * lat_rx[slot, srows[g], :].astype(F32)
                )
                acc[g] = acc[g] + live * tot[g]
        blocks = []
        for g in range(groups):
            entry = (state[g] + jnp.exp(acc[g]) * start[d][g]).astype(BF16)
            pieces = [
                entry if k == g else jnp.zeros((STATE, repeat_cols), BF16) for k in range(groups)
            ]
            blocks.append(jnp.concatenate(pieces, axis=1) if groups > 1 else entry)
        entry_all = jnp.concatenate(blocks, axis=0) if groups > 1 else blocks[0]
        mixed_y = mixed_y + reach[:, d * head_cols:(d + 1) * head_cols] * dot(lat_c, entry_all)
    gated = mixed_y * gate_act
    og_row = flat_row(og[...].astype(F32))
    for g in range(groups):
        part_g = gated[:, g * repeat_cols:(g + 1) * repeat_cols]
        ms = jnp.mean(part_g * part_g, axis=-1, keepdims=True)
        nrm[:, g * repeat_cols:(g + 1) * repeat_cols] = (
            part_g * lax.rsqrt(ms + GROUP_EPS) * og_row[:, g * repeat_cols:(g + 1) * repeat_cols]
        ).astype(BF16)

    nm = []
    for d in range(1, n_tp):
        u = lax.rem(t + d, n_tp)
        c = remote(nrm.at[pl.ds(pl.multiple_of(u * rows, 16), rows)], nrm_rx.at[d],
                   nm_send.at[d], nm_recv.at[d], {"sp": s, "tp": u})
        c.start()
        nm.append(c)
    loads[15].wait()

    def out_rows(u):
        return wout[pl.ds(pl.multiple_of(u * head_cols, 16), head_cols), :]

    branch = dot(nrm[own_rows, :], out_rows(t))
    for d in range(1, n_tp):
        nm[d - 1].wait_recv()
        branch = branch + dot(nrm_rx[d], out_rows(lax.rem(t + n_tp - d, n_tp)))
    out_v[...] = (lat[own_rows, :].astype(F32) + gate_row * branch).astype(BF16)
    final = pltpu.make_async_copy(out_v, out_h, out_sem)
    final.start()

    for c in tok + ctx_halo + cm + lm + nm:
        c.wait_send()

    @pl.when(t == n_tp - 1)
    def _():
        for c in low:
            c.wait_send()

    @pl.when(t == 0)
    def _():
        for c in high:
            c.wait_send()

    for d in range(1, n):
        other = lax.rem(rank + d, n)
        guarded(full, other < reducers, rs[d - 1].wait_send)

    def ag_done():
        for c in ag:
            c.wait_send()

    guarded(full, rank < reducers, ag_done)
    final.wait()


def local(
    latent, cond, context, context_cond, modulation, norm_gain, w_x, w_gate, w_b, w_c, w_dt,
    conv_x, conv_b, conv_c, decay_rate, decay_extra, out_gain, w_out,
):
    n_sp = lax.axis_size("sp")
    n_tp = lax.axis_size("tp")
    n = n_sp * n_tp
    rows, width = latent.shape
    length = decay_extra.shape[0]
    ctx_len = context.shape[0]
    mod_cols = modulation.shape[1]
    head_cols = w_x.shape[1]
    state_cols = w_b.shape[1]
    groups = state_cols // STATE
    repeat_cols = head_cols // groups
    reducers = max(m for m in range(1, n + 1) if mod_cols % (LANES * m) == 0)
    chunk = mod_cols // reducers

    args = (
        cond.reshape(-1, LANES), latent, context, modulation, norm_gain.reshape(-1, LANES),
        w_x, w_gate, w_b, w_c, jnp.swapaxes(w_dt, 1, 2), conv_x, conv_b, conv_c,
        decay_extra.T, out_gain.reshape(-1, LANES), w_out, context_cond.reshape(-1, LANES),
        decay_rate,
    )
    V = pltpu.VMEM
    D = pltpu.SemaphoreType.DMA
    held = [args[i] for i in (0, 3, 4, 5, 6, 7, 8, 9, 10, 11, 12, 13, 14, 15, 16, 17)]
    msg = (groups * STATE + 16, repeat_cols)
    scratch = [V(a.shape, a.dtype) for a in held] + [
        V((2, width // LANES, LANES), F32),
        V((LANES, width), BF16),
        V((length, width), BF16),
        V((ctx_len, width), BF16),
        V((HALO, width), BF16),
        V((HALO, width), BF16),
        V((HALO, width), BF16),
        V((HALO, width), BF16),
        V((reducers, 2, chunk), F32),
        V((n, 2, chunk), F32),
        V((reducers, 2, chunk), F32),
        V((length + HALO, width), BF16),
        V((ctx_len + HALO, width), BF16),
        V((n_sp, 2) + msg, BF16),
        V((2,) + msg, BF16),
        V((n_sp,) + msg, BF16),
        V((length, head_cols), F32),
        V((length, head_cols), BF16),
        V((n_tp, rows, head_cols), BF16),
        V((rows, width), BF16),
        D((len(args),)),
        D((4 + 2 * n_tp,)),
        D((4,)),
        D((n_tp,)), D((n_tp,)),
        D((n,)), D((n,)), D((n,)), D((n,)),
        D((n_sp,)), D((n_sp,)), D((n_sp,)), D((n_sp,)),
        D((n_tp,)), D((n_tp,)),
        D,
    ]
    return pl.pallas_call(
        functools.partial(mixer_kernel, n_sp, n_tp, reducers),
        out_shape=jax.ShapeDtypeStruct((rows, width), BF16),
        in_specs=[pl.BlockSpec(memory_space=pl.ANY)] * len(args),
        out_specs=pl.BlockSpec(memory_space=pl.ANY),
        scratch_shapes=scratch,
        compiler_params=pltpu.CompilerParams(
            collective_id=0, has_side_effects=True, vmem_limit_bytes=60 * 1024 * 1024
        ),
    )(*args)


def solution(mesh):
    in_specs = (
        P(("dp", "sp", "tp"), None),
        P("dp"),
        P(("dp", "sp"), None),
        P(),
        P(("sp", "tp"), None),
        P(),
        P(None, "tp"),
        P(None, "tp"),
        P(None, "tp"),
        P(None, "tp"),
        P(None, None, "tp"),
        P(None, "tp"),
        P(None, "tp"),
        P(None, "tp"),
        P(None, "tp"),
        P(("dp", "sp"), "tp"),
        P("tp"),
        P(),
    )
    out_specs = P(("dp", "sp", "tp"), None)
    return jax.shard_map(local, mesh=mesh, in_specs=in_specs, out_specs=out_specs, check_vma=False)
```

```python
import functools

import jax
import jax.numpy as jnp
from jax import lax
from jax.experimental import pallas as pl
from jax.experimental.pallas import tpu as pltpu
from jax.sharding import PartitionSpec as P

HEAD_DIM = 64
STATE = 64
HALO = 16
LANES = 128
ROW_EPS = 1e-06
GROUP_EPS = 1e-05
HIGHEST = lax.Precision.HIGHEST
MESH = pl.DeviceIdType.MESH
F32 = jnp.float32
BF16 = jnp.bfloat16


def silu(v):
    return v / (1.0 + jnp.exp(-v))


def softplus(v):
    return jnp.maximum(v, 0.0) + jnp.log1p(jnp.exp(-jnp.abs(v)))


def dot(a, b):
    return jnp.dot(a, b, preferred_element_type=F32)


def dot_nt(a, b):
    return lax.dot_general(a, b, (((1,), (1,)), ((), ())), preferred_element_type=F32)


def dot_tn(a, b):
    return lax.dot_general(a, b, (((0,), (0,)), ((), ())), preferred_element_type=F32)


def split(v):
    hi = v.astype(BF16)
    return hi, (v - hi.astype(F32)).astype(BF16)


def iota(shape, dim):
    return lax.broadcasted_iota(jnp.int32, shape, dim)


def flat_row(tiled):
    return jnp.concatenate([tiled[i:i + 1] for i in range(tiled.shape[0])], axis=1)


def own_cond(rows_ref, k, rank, share):
    if share % LANES == 0:
        count = share // LANES
        return jnp.concatenate(
            [rows_ref[k, pl.ds(rank * count + i, 1), :] for i in range(count)], axis=1
        )
    per = LANES // share
    row = jnp.broadcast_to(rows_ref[k, pl.ds(rank // per, 1), :], (8, LANES))
    moved = pltpu.roll(row, lax.rem(LANES - lax.rem(rank, per) * share, LANES), 1)
    return moved[0:1, :share]


def guarded(always, cond, body):
    if always:
        body()
    else:
        pl.when(cond)(body)


def mixer_kernel(
    n_sp, n_tp, reducers,
    cond_h, latent_h, context_h, modulation_h, gain_h, wx_h, wg_h, wb_h, wc_h, wdt_h,
    cx_h, cb_h, cc_h, extra_h, og_h, wout_h, ccond_h, rate_h,
    out_h,
    cond, mod_w, gain, wx, wg, wb, wc, wdt, cx, cb, cc, extra, og, wout, ccond, rate,
    cond_rows, wdt_all,
    lat, ctx, lat_prev, lat_next, ctx_prev, ctx_next,
    part, part_rx, mod_full, hid_l, hid_c,
    ctx_st, lat_st, ent_tx, ent_rx, y_loc, nrm, nrm_rx, out_v,
    in_sem, halo_send, halo_recv, tok_send, tok_recv,
    rs_send, rs_recv, ag_send, ag_recv,
    cm_send, cm_recv, lm_send, lm_recv, em_send, em_recv, nm_send, nm_recv, out_sem,
):
    s = lax.axis_index("sp")
    t = lax.axis_index("tp")
    n = n_sp * n_tp
    rank = s * n_tp + t
    rows = latent_h.shape[0]
    length = lat.shape[0]
    ctx_len = ctx.shape[0]
    width = lat.shape[1]
    head_cols = wx.shape[1]
    state_cols = wb.shape[1]
    heads = head_cols // HEAD_DIM
    groups = state_cols // STATE
    repeat_cols = head_cols // groups
    chunk = part.shape[2]

    barrier = pltpu.get_barrier_semaphore()

    def group_peer(d):
        other = lax.rem(rank + d, n)
        return {"sp": other // n_tp, "tp": lax.rem(other, n_tp)}

    for d in range(1, n):
        pl.semaphore_signal(barrier, inc=1, device_id=group_peer(d), device_id_type=MESH)

    own_rows = pl.ds(pl.multiple_of(t * rows, 16), rows)
    pairs = [
        (cond_h, cond), (modulation_h, mod_w), (latent_h, lat.at[own_rows]), (context_h, ctx),
        (gain_h, gain), (wx_h, wx), (wb_h, wb), (wdt_h, wdt), (cx_h, cx), (cb_h, cb),
        (extra_h, extra), (wc_h, wc), (cc_h, cc), (wg_h, wg), (og_h, og), (wout_h, wout),
        (ccond_h, ccond), (rate_h, rate),
    ]
    loads = [pltpu.make_async_copy(a, b, in_sem.at[i]) for i, (a, b) in enumerate(pairs)]
    for c in loads:
        c.start()
    pl.semaphore_wait(barrier, n - 1)

    sends = []

    def remote(src, dst, ssem, rsem, device):
        return pltpu.make_async_remote_copy(
            src_ref=src, dst_ref=dst, send_sem=ssem, recv_sem=rsem,
            device_id=device, device_id_type=MESH,
        )

    after = lax.rem(s + 1, n_sp)
    before = lax.rem(s + n_sp - 1, n_sp)
    tok = []
    for d in range(1, n_tp):
        c = remote(latent_h, lat.at[own_rows], tok_send.at[d], tok_recv.at[d],
                   {"sp": s, "tp": lax.rem(t + d, n_tp)})
        c.start()
        tok.append(c)
    ctx_halo = [
        remote(context_h.at[pl.ds(ctx_len - HALO, HALO)], ctx_prev, halo_send.at[0],
               halo_recv.at[0], {"sp": after, "tp": t}),
        remote(context_h.at[pl.ds(0, HALO)], ctx_next, halo_send.at[1], halo_recv.at[1],
               {"sp": before, "tp": t}),
    ]
    for c in ctx_halo:
        c.start()
    low = [remote(latent_h.at[pl.ds(rows - HALO, HALO)], lat_prev, halo_send.at[4 + u],
                  halo_recv.at[2], {"sp": after, "tp": u}) for u in range(n_tp)]
    high = [remote(latent_h.at[pl.ds(0, HALO)], lat_next, halo_send.at[4 + n_tp + u],
                   halo_recv.at[3], {"sp": before, "tp": u}) for u in range(n_tp)]

    @pl.when(t == n_tp - 1)
    def _():
        for c in low:
            c.start()

    @pl.when(t == 0)
    def _():
        for c in high:
            c.start()

    loads[0].wait()
    loads[16].wait()
    cond_rows[0] = silu(cond[...].astype(F32))
    cond_rows[1] = silu(ccond[...].astype(F32))
    own = [own_cond(cond_rows, k, rank, mod_w.shape[0]) for k in range(2)]
    pick = iota((16, mod_w.shape[0]), 0)
    cols = jnp.where(pick == 0, own[0], jnp.where(pick == 1, own[1], 0.0)).astype(BF16)
    loads[1].wait()
    full = reducers == n
    partial = dot(cols, mod_w[...])
    for i in range(reducers):
        part[i] = partial[0:2, i * chunk:(i + 1) * chunk]
    rs = []
    for d in range(1, n):
        other = lax.rem(rank + d, n)
        rs.append(remote(part.at[lax.rem(other, reducers)], part_rx.at[d], rs_send.at[d],
                         rs_recv.at[d], group_peer(d)))
        guarded(full, other < reducers, rs[-1].start)

    for i in (2, 3, 4):
        loads[i].wait()
    ag = [remote(mod_full.at[lax.rem(rank, reducers)], mod_full.at[lax.rem(rank, reducers)],
                 ag_send.at[d], ag_recv.at[d], group_peer(d)) for d in range(1, n)]

    def reduce_chunk():
        total = part[lax.rem(rank, reducers)]
        for d in range(1, n):
            rs[d - 1].wait_recv()
            total = total + part_rx[d]
        mod_full[lax.rem(rank, reducers)] = total
        for c in ag:
            c.start()

    guarded(full, rank < reducers, reduce_chunk)

    def normed_rows(halo_prev, halo_next, body):
        edge = jnp.where(
            iota((HALO, width), 0) == 0,
            halo_next[...].astype(F32),
            halo_prev[...].astype(F32),
        )
        values = jnp.concatenate([edge, body[...].astype(F32)], axis=0)
        return values, lax.rsqrt(jnp.mean(values * values, axis=-1, keepdims=True) + ROW_EPS)

    for c in ctx_halo:
        c.wait_recv()
    ctx_vals, ctx_rs = normed_rows(ctx_prev, ctx_next, ctx)
    gain_row = flat_row(gain[...].astype(F32))
    for i in (7, 10, 17):
        loads[i].wait()
    spare = LANES - 2 * heads
    wdt_all[...] = jnp.concatenate(
        [wdt[0].astype(F32), wdt[1].astype(F32), jnp.zeros((spare, width), F32)], axis=0
    ).astype(BF16)
    extra_all = jnp.transpose(
        jnp.concatenate([extra[...], extra[...], jnp.zeros((spare, length), F32)], axis=0)
    )
    rate_row = -jnp.concatenate([rate[0:1, :], rate[1:2, :], jnp.zeros((1, spare), F32)], axis=1)

    for d in range(1, n):
        source = lax.rem(rank + n - d, n)
        guarded(full, source < reducers, ag[d - 1].wait_recv)
    mod_rows = jnp.concatenate([mod_full[i] for i in range(reducers)], axis=1)
    shift = mod_rows[:, :width]
    scale = mod_rows[:, width:2 * width]
    gate_row = mod_rows[0:1, 2 * width:]

    def conv(z, taps_ref):
        total_rows = z.shape[0]
        has_prev = jnp.where(s > 0, 1, 0)
        has_next = jnp.where(s < n_sp - 1, 1, 0)
        r = iota(z.shape, 0)
        keep = jnp.where(r == 0, has_next, jnp.where(r < HALO, has_prev, 1))
        z = jnp.where(keep > 0, z, 0.0)
        taps = taps_ref[...].astype(F32)
        u = (
            taps[0:1] * pltpu.roll(z, 2, 0)
            + taps[1:2] * pltpu.roll(z, 1, 0)
            + taps[2:3] * z
            + taps[3:4] * pltpu.roll(z, total_rows - 1, 0)
        )
        return silu(u[HALO:])

    lane_row = iota((1, LANES), 1)
    expander = (
        iota((LANES, 2 * head_cols), 0) == iota((LANES, 2 * head_cols), 1) // HEAD_DIM
    ).astype(F32).astype(BF16)

    def expand(v):
        hi, lo = split(v)
        return dot(hi, expander) + dot(lo, expander)

    def decay_run(log_decay):
        size = log_decay.shape[0]
        i = iota((size, size), 0)
        j = iota((size, size), 1)
        pre = jnp.dot((j <= i).astype(F32), log_decay, precision=HIGHEST,
                      preferred_element_type=F32)
        total = pre[size - 1:size]
        suf = total - pre + log_decay
        return jnp.where(lane_row < heads, pre, suf), total

    blocks = [(d, g, (d * groups + g) % n_sp) for d in range(2) for g in range(groups)]

    def summarize(held, xs, bm, dt, run, total):
        weight = expand(jnp.exp(total - run) * dt)
        thi, tlo = split(jnp.broadcast_to(total, (16, LANES)))
        tail = jnp.where(
            iota((16, 2 * head_cols), 0) == 0, dot(thi, expander), dot(tlo, expander)
        ).astype(BF16)
        states = [
            dot_tn(bm, (xs * weight[:, d * head_cols:(d + 1) * head_cols]).astype(BF16))
            for d in range(2)
        ]
        for b, (d, g, _) in enumerate(blocks):
            lo = g * repeat_cols
            held[b, s, 0:STATE, :] = states[d][
                g * STATE:(g + 1) * STATE, lo:lo + repeat_cols
            ].astype(BF16)
            lo = d * head_cols + lo
            held[b, s, STATE:, :] = tail[:, lo:lo + repeat_cols]

    def to_owner(held, b, source, ssem, rsem):
        return remote(held.at[b, source], held.at[b, source], ssem.at[b],
                      rsem.at[b * n_sp + source], {"sp": blocks[b][2], "tp": t})

    def send_blocks(held, ssem, rsem):
        for b, (_, _, owner) in enumerate(blocks):
            pl.when(s != owner)(to_owner(held, b, s, ssem, rsem).start)

    hid_c[...] = (
        ctx_vals * ctx_rs * gain_row * (1.0 + scale[1:2]) + shift[1:2]
    ).astype(BF16)
    for i in (5, 6, 8, 9):
        loads[i].wait()
    ctx_x = conv(dot(hid_c[...], wx[...]), cx)
    ctx_b = conv(dot(hid_c[...], wb[...]), cb).astype(BF16)
    ctx_dt = softplus(dot_nt(hid_c[HALO:, :], wdt_all[...]))
    ctx_run, ctx_total = decay_run(rate_row * ctx_dt)
    summarize(ctx_st, ctx_x, ctx_b, ctx_dt, ctx_run, ctx_total)
    send_blocks(ctx_st, cm_send, cm_recv)

    for c in tok:
        c.wait_recv()
    low[0].wait_recv()
    high[0].wait_recv()
    lat_vals, lat_rs = normed_rows(lat_prev, lat_next, lat)
    hid_l[...] = (
        lat_vals * lat_rs * gain_row * (1.0 + scale[0:1]) + shift[0:1]
    ).astype(BF16)
    lat_x = conv(dot(hid_l[...], wx[...]), cx)
    lat_b = conv(dot(hid_l[...], wb[...]), cb).astype(BF16)
    dt = softplus(dot_nt(hid_l[HALO:, :], wdt_all[...]))
    run, total = decay_run(rate_row * dt + extra_all)
    summarize(lat_st, lat_x, lat_b, dt, run, total)
    send_blocks(lat_st, lm_send, lm_recv)

    loads[11].wait()
    loads[12].wait()
    lat_c = conv(dot(hid_l[...], wc[...]), cc).astype(BF16)
    run_t = jnp.transpose(run)
    dt_t = jnp.transpose(dt)
    i_pos = iota((length, length), 0)
    j_pos = iota((length, length), 1)
    lat_xb = lat_x.astype(BF16)
    state_lane = iota((length, state_cols), 1) // STATE
    pair_lane = iota((length, LANES), 1)
    zero_b = jnp.zeros((), BF16)
    per_group = heads // groups
    affinity = [
        dot_nt(jnp.where(state_lane == g, lat_c, zero_b), lat_b) for g in range(groups)
    ]

    def block_weights(h):
        ahead = heads + h
        gap = jnp.where(
            j_pos <= i_pos,
            run[:, h:h + 1] - run_t[h:h + 1, :],
            run[:, ahead:ahead + 1] - run_t[ahead:ahead + 1, :],
        )
        step = jnp.where(j_pos <= i_pos, dt_t[h:h + 1, :], 0.0) + jnp.where(
            j_pos >= i_pos, dt_t[ahead:ahead + 1, :], 0.0
        )
        return (affinity[h // per_group] * jnp.exp(gap) * step).astype(BF16)

    for q in range(heads // 2):
        both = lat_xb[:, q * LANES:(q + 1) * LANES]
        y_loc[:, q * LANES:(q + 1) * LANES] = dot(
            jnp.concatenate([block_weights(2 * q), block_weights(2 * q + 1)], axis=1),
            jnp.concatenate(
                [
                    jnp.where(pair_lane < HEAD_DIM, both, zero_b),
                    jnp.where(pair_lane >= HEAD_DIM, both, zero_b),
                ],
                axis=0,
            ),
        )
    reach = expand(jnp.exp(run))
    loads[13].wait()
    loads[14].wait()
    gate_act = silu(dot(hid_l[HALO:, :], wg[...]))

    def entry_copy(b, k):
        return remote(ent_tx.at[b, k], ent_rx.at[b], em_send.at[b * n_sp + k], em_recv.at[b],
                      {"sp": k, "tp": t})

    def growth(held, b, k):
        tail = held[b, k, STATE:, :].astype(F32)
        return jnp.exp(tail[0:1] + tail[1:2])

    def scan_block(b, d, owner):
        order = list(range(n_sp)) if d == 0 else list(range(n_sp - 1, -1, -1))
        for k in range(n_sp):
            if k != owner:
                to_owner(ctx_st, b, k, cm_send, cm_recv).wait_recv()
        state = jnp.zeros((STATE, repeat_cols), F32)
        for k in order:
            state = growth(ctx_st, b, k) * state + ctx_st[b, k, 0:STATE, :].astype(F32)
        for k in range(n_sp):
            if k != owner:
                to_owner(lat_st, b, k, lm_send, lm_recv).wait_recv()
        for k in order:
            entry = state.astype(BF16)
            if k == owner:
                ent_rx[b] = entry
            else:
                ent_tx[b, k] = entry
                entry_copy(b, k).start()
            state = growth(lat_st, b, k) * state + lat_st[b, k, 0:STATE, :].astype(F32)

    for b, (d, g, owner) in enumerate(blocks):
        pl.when(s == owner)(functools.partial(scan_block, b, d, owner))
    for b, (d, g, owner) in enumerate(blocks):
        pl.when(s != owner)(entry_copy(b, s).wait_recv)
    mixed_y = y_loc[...]
    zero_block = jnp.zeros((STATE, repeat_cols), BF16)
    for d in range(2):
        entry_all = jnp.concatenate(
            [
                jnp.concatenate(
                    [ent_rx[d * groups + g] if k == g else zero_block for k in range(groups)],
                    axis=1,
                )
                for g in range(groups)
            ],
            axis=0,
        )
        mixed_y = mixed_y + reach[:, d * head_cols:(d + 1) * head_cols] * dot(lat_c, entry_all)
    gated = mixed_y * gate_act
    og_row = flat_row(og[...].astype(F32))
    for g in range(groups):
        part_g = gated[:, g * repeat_cols:(g + 1) * repeat_cols]
        ms = jnp.mean(part_g * part_g, axis=-1, keepdims=True)
        nrm[:, g * repeat_cols:(g + 1) * repeat_cols] = (
            part_g * lax.rsqrt(ms + GROUP_EPS) * og_row[:, g * repeat_cols:(g + 1) * repeat_cols]
        ).astype(BF16)

    nm = []
    for d in range(1, n_tp):
        u = lax.rem(t + d, n_tp)
        c = remote(nrm.at[pl.ds(pl.multiple_of(u * rows, 16), rows)], nrm_rx.at[d],
                   nm_send.at[d], nm_recv.at[d], {"sp": s, "tp": u})
        c.start()
        nm.append(c)
    loads[15].wait()

    def out_rows(u):
        return wout[pl.ds(pl.multiple_of(u * head_cols, 16), head_cols), :]

    branch = dot(nrm[own_rows, :], out_rows(t))
    for d in range(1, n_tp):
        nm[d - 1].wait_recv()
        branch = branch + dot(nrm_rx[d], out_rows(lax.rem(t + n_tp - d, n_tp)))
    out_v[...] = (lat[own_rows, :].astype(F32) + gate_row * branch).astype(BF16)
    final = pltpu.make_async_copy(out_v, out_h, out_sem)
    final.start()

    for c in tok + ctx_halo + nm:
        c.wait_send()

    def sent(b, owner):
        to_owner(ctx_st, b, s, cm_send, cm_recv).wait_send()
        to_owner(lat_st, b, s, lm_send, lm_recv).wait_send()

    def handed(b, owner):
        for k in range(n_sp):
            if k != owner:
                entry_copy(b, k).wait_send()

    for b, (d, g, owner) in enumerate(blocks):
        pl.when(s != owner)(functools.partial(sent, b, owner))
        pl.when(s == owner)(functools.partial(handed, b, owner))

    @pl.when(t == n_tp - 1)
    def _():
        for c in low:
            c.wait_send()

    @pl.when(t == 0)
    def _():
        for c in high:
            c.wait_send()

    for d in range(1, n):
        other = lax.rem(rank + d, n)
        guarded(full, other < reducers, rs[d - 1].wait_send)

    def ag_done():
        for c in ag:
            c.wait_send()

    guarded(full, rank < reducers, ag_done)
    final.wait()


def local(
    latent, cond, context, context_cond, modulation, norm_gain, w_x, w_gate, w_b, w_c, w_dt,
    conv_x, conv_b, conv_c, decay_rate, decay_extra, out_gain, w_out,
):
    n_sp = lax.axis_size("sp")
    n_tp = lax.axis_size("tp")
    n = n_sp * n_tp
    rows, width = latent.shape
    length = decay_extra.shape[0]
    ctx_len = context.shape[0]
    mod_cols = modulation.shape[1]
    head_cols = w_x.shape[1]
    state_cols = w_b.shape[1]
    groups = state_cols // STATE
    repeat_cols = head_cols // groups
    reducers = max(m for m in range(1, n + 1) if mod_cols % (LANES * m) == 0)
    chunk = mod_cols // reducers

    args = (
        cond.reshape(-1, LANES), latent, context, modulation, norm_gain.reshape(-1, LANES),
        w_x, w_gate, w_b, w_c, jnp.swapaxes(w_dt, 1, 2), conv_x, conv_b, conv_c,
        decay_extra.T, out_gain.reshape(-1, LANES), w_out, context_cond.reshape(-1, LANES),
        decay_rate,
    )
    V = pltpu.VMEM
    D = pltpu.SemaphoreType.DMA
    held = [args[i] for i in (0, 3, 4, 5, 6, 7, 8, 9, 10, 11, 12, 13, 14, 15, 16, 17)]
    count = 2 * groups
    scratch = [V(a.shape, a.dtype) for a in held] + [
        V((2, width // LANES, LANES), F32),
        V((LANES, width), BF16),
        V((length, width), BF16),
        V((ctx_len, width), BF16),
        V((HALO, width), BF16),
        V((HALO, width), BF16),
        V((HALO, width), BF16),
        V((HALO, width), BF16),
        V((reducers, 2, chunk), F32),
        V((n, 2, chunk), F32),
        V((reducers, 2, chunk), F32),
        V((length + HALO, width), BF16),
        V((ctx_len + HALO, width), BF16),
        V((count, n_sp, STATE + 16, repeat_cols), BF16),
        V((count, n_sp, STATE + 16, repeat_cols), BF16),
        V((count, n_sp, STATE, repeat_cols), BF16),
        V((count, STATE, repeat_cols), BF16),
        V((length, head_cols), F32),
        V((length, head_cols), BF16),
        V((n_tp, rows, head_cols), BF16),
        V((rows, width), BF16),
        D((len(args),)),
        D((4 + 2 * n_tp,)),
        D((4,)),
        D((n_tp,)), D((n_tp,)),
        D((n,)), D((n,)), D((n,)), D((n,)),
        D((count,)), D((count * n_sp,)), D((count,)), D((count * n_sp,)),
        D((count * n_sp,)), D((count,)),
        D((n_tp,)), D((n_tp,)),
        D,
    ]
    return pl.pallas_call(
        functools.partial(mixer_kernel, n_sp, n_tp, reducers),
        out_shape=jax.ShapeDtypeStruct((rows, width), BF16),
        in_specs=[pl.BlockSpec(memory_space=pl.ANY)] * len(args),
        out_specs=pl.BlockSpec(memory_space=pl.ANY),
        scratch_shapes=scratch,
        compiler_params=pltpu.CompilerParams(
            collective_id=0, has_side_effects=True, vmem_limit_bytes=60 * 1024 * 1024
        ),
    )(*args)


def solution(mesh):
    in_specs = (
        P(("dp", "sp", "tp"), None),
        P("dp"),
        P(("dp", "sp"), None),
        P(),
        P(("sp", "tp"), None),
        P(),
        P(None, "tp"),
        P(None, "tp"),
        P(None, "tp"),
        P(None, "tp"),
        P(None, None, "tp"),
        P(None, "tp"),
        P(None, "tp"),
        P(None, "tp"),
        P(None, "tp"),
        P(("dp", "sp"), "tp"),
        P("tp"),
        P(),
    )
    out_specs = P(("dp", "sp", "tp"), None)
    return jax.shard_map(local, mesh=mesh, in_specs=in_specs, out_specs=out_specs, check_vma=False)
```

```python
import functools

import jax
import jax.numpy as jnp
from jax import lax
from jax.experimental import pallas as pl
from jax.experimental.pallas import tpu as pltpu
from jax.sharding import PartitionSpec as P

HEAD_DIM = 64
STATE = 64
HALO = 16
LANES = 128
ROW_EPS = 1e-06
GROUP_EPS = 1e-05
HIGHEST = lax.Precision.HIGHEST
MESH = pl.DeviceIdType.MESH
F32 = jnp.float32
BF16 = jnp.bfloat16


def silu(v):
    return v / (1.0 + jnp.exp(-v))


def softplus(v):
    return jnp.maximum(v, 0.0) + jnp.log1p(jnp.exp(-jnp.abs(v)))


def dot(a, b):
    return jnp.dot(a, b, preferred_element_type=F32)


def dot_nt(a, b):
    return lax.dot_general(a, b, (((1,), (1,)), ((), ())), preferred_element_type=F32)


def dot_tn(a, b):
    return lax.dot_general(a, b, (((0,), (0,)), ((), ())), preferred_element_type=F32)


def split(v):
    hi = v.astype(BF16)
    return hi, (v - hi.astype(F32)).astype(BF16)


def iota(shape, dim):
    return lax.broadcasted_iota(jnp.int32, shape, dim)


def flat_row(tiled):
    return jnp.concatenate([tiled[i:i + 1] for i in range(tiled.shape[0])], axis=1)


def own_cond(rows_ref, k, rank, share):
    if share % LANES == 0:
        count = share // LANES
        return jnp.concatenate(
            [rows_ref[k, pl.ds(rank * count + i, 1), :] for i in range(count)], axis=1
        )
    per = LANES // share
    row = jnp.broadcast_to(rows_ref[k, pl.ds(rank // per, 1), :], (8, LANES))
    moved = pltpu.roll(row, lax.rem(LANES - lax.rem(rank, per) * share, LANES), 1)
    return moved[0:1, :share]


def guarded(always, cond, body):
    if always:
        body()
    else:
        pl.when(cond)(body)


def mixer_kernel(
    n_sp, n_tp, reducers,
    cond_h, latent_h, context_h, modulation_h, gain_h, wx_h, wg_h, wb_h, wc_h, wdt_h,
    cx_h, cb_h, cc_h, extra_h, og_h, wout_h, ccond_h, rate_h,
    out_h,
    cond, mod_w, gain, wx, wg, wb, wc, wdt, cx, cb, cc, extra, og, wout, ccond, rate,
    cond_rows, wdt_all,
    lat, ctx, lat_prev, lat_next, ctx_prev, ctx_next,
    part, part_rx, mod_full, hid_l, hid_c,
    ctx_st, lat_st, ent_tx, ent_rx, y_loc, nrm, nrm_rx, out_v,
    in_sem, halo_send, halo_recv, tok_send, tok_recv,
    rs_send, rs_recv, ag_send, ag_recv,
    cm_send, cm_recv, lm_send, lm_recv, em_send, em_recv, nm_send, nm_recv, out_sem,
):
    s = lax.axis_index("sp")
    t = lax.axis_index("tp")
    n = n_sp * n_tp
    rank = s * n_tp + t
    rows = latent_h.shape[0]
    length = lat.shape[0]
    ctx_len = ctx.shape[0]
    width = lat.shape[1]
    head_cols = wx.shape[1]
    state_cols = wb.shape[1]
    heads = head_cols // HEAD_DIM
    groups = state_cols // STATE
    repeat_cols = head_cols // groups
    chunk = part.shape[2]

    barrier = pltpu.get_barrier_semaphore()

    def group_peer(d):
        other = lax.rem(rank + d, n)
        return {"sp": other // n_tp, "tp": lax.rem(other, n_tp)}

    for d in range(1, n):
        pl.semaphore_signal(barrier, inc=1, device_id=group_peer(d), device_id_type=MESH)

    own_rows = pl.ds(pl.multiple_of(t * rows, 16), rows)
    pairs = [
        (cond_h, cond), (modulation_h, mod_w), (latent_h, lat.at[own_rows]), (context_h, ctx),
        (gain_h, gain), (wx_h, wx), (wb_h, wb), (wdt_h, wdt), (cx_h, cx), (cb_h, cb),
        (extra_h, extra), (wc_h, wc), (cc_h, cc), (wg_h, wg), (og_h, og), (wout_h, wout),
        (ccond_h, ccond), (rate_h, rate),
    ]
    loads = [pltpu.make_async_copy(a, b, in_sem.at[i]) for i, (a, b) in enumerate(pairs)]
    for c in loads:
        c.start()
    pl.semaphore_wait(barrier, n - 1)

    sends = []

    def remote(src, dst, ssem, rsem, device):
        return pltpu.make_async_remote_copy(
            src_ref=src, dst_ref=dst, send_sem=ssem, recv_sem=rsem,
            device_id=device, device_id_type=MESH,
        )

    after = lax.rem(s + 1, n_sp)
    before = lax.rem(s + n_sp - 1, n_sp)
    loads[0].wait()
    loads[16].wait()
    cond_rows[0] = silu(cond[...].astype(F32))
    cond_rows[1] = silu(ccond[...].astype(F32))
    own = [own_cond(cond_rows, k, rank, mod_w.shape[0]) for k in range(2)]
    pick = iota((16, mod_w.shape[0]), 0)
    cols = jnp.where(pick == 0, own[0], jnp.where(pick == 1, own[1], 0.0)).astype(BF16)
    loads[1].wait()
    full = reducers == n
    partial = dot(cols, mod_w[...])
    for i in range(reducers):
        part[i] = partial[0:2, i * chunk:(i + 1) * chunk]
    rs = []
    for d in range(1, n):
        other = lax.rem(rank + d, n)
        rs.append(remote(part.at[lax.rem(other, reducers)], part_rx.at[d], rs_send.at[d],
                         rs_recv.at[d], group_peer(d)))
        guarded(full, other < reducers, rs[-1].start)

    tok = []
    for d in range(1, n_tp):
        c = remote(latent_h, lat.at[own_rows], tok_send.at[d], tok_recv.at[d],
                   {"sp": s, "tp": lax.rem(t + d, n_tp)})
        c.start()
        tok.append(c)
    ctx_halo = [
        remote(context_h.at[pl.ds(ctx_len - HALO, HALO)], ctx_prev, halo_send.at[0],
               halo_recv.at[0], {"sp": after, "tp": t}),
        remote(context_h.at[pl.ds(0, HALO)], ctx_next, halo_send.at[1], halo_recv.at[1],
               {"sp": before, "tp": t}),
    ]
    for c in ctx_halo:
        c.start()
    low = [remote(latent_h.at[pl.ds(rows - HALO, HALO)], lat_prev, halo_send.at[4 + u],
                  halo_recv.at[2], {"sp": after, "tp": u}) for u in range(n_tp)]
    high = [remote(latent_h.at[pl.ds(0, HALO)], lat_next, halo_send.at[4 + n_tp + u],
                   halo_recv.at[3], {"sp": before, "tp": u}) for u in range(n_tp)]

    @pl.when(t == n_tp - 1)
    def _():
        for c in low:
            c.start()

    @pl.when(t == 0)
    def _():
        for c in high:
            c.start()

    for i in (2, 3, 4):
        loads[i].wait()
    ag = [remote(mod_full.at[lax.rem(rank, reducers)], mod_full.at[lax.rem(rank, reducers)],
                 ag_send.at[d], ag_recv.at[d], group_peer(d)) for d in range(1, n)]

    def reduce_chunk():
        total = part[lax.rem(rank, reducers)]
        for d in range(1, n):
            rs[d - 1].wait_recv()
            total = total + part_rx[d]
        mod_full[lax.rem(rank, reducers)] = total
        for c in ag:
            c.start()

    guarded(full, rank < reducers, reduce_chunk)

    def normed_rows(halo_prev, halo_next, body):
        edge = jnp.where(
            iota((HALO, width), 0) == 0,
            halo_next[...].astype(F32),
            halo_prev[...].astype(F32),
        )
        values = jnp.concatenate([edge, body[...].astype(F32)], axis=0)
        return values, lax.rsqrt(jnp.mean(values * values, axis=-1, keepdims=True) + ROW_EPS)

    for c in ctx_halo:
        c.wait_recv()
    ctx_vals, ctx_rs = normed_rows(ctx_prev, ctx_next, ctx)
    gain_row = flat_row(gain[...].astype(F32))
    for i in (7, 10, 17):
        loads[i].wait()
    spare = LANES - 2 * heads
    wdt_all[...] = jnp.concatenate(
        [wdt[0].astype(F32), wdt[1].astype(F32), jnp.zeros((spare, width), F32)], axis=0
    ).astype(BF16)
    extra_all = jnp.transpose(
        jnp.concatenate([extra[...], extra[...], jnp.zeros((spare, length), F32)], axis=0)
    )
    rate_row = -jnp.concatenate([rate[0:1, :], rate[1:2, :], jnp.zeros((1, spare), F32)], axis=1)

    for d in range(1, n):
        source = lax.rem(rank + n - d, n)
        guarded(full, source < reducers, ag[d - 1].wait_recv)
    mod_rows = jnp.concatenate([mod_full[i] for i in range(reducers)], axis=1)
    shift = mod_rows[:, :width]
    scale = mod_rows[:, width:2 * width]
    gate_row = mod_rows[0:1, 2 * width:]

    def conv(z, taps_ref):
        total_rows = z.shape[0]
        has_prev = jnp.where(s > 0, 1, 0)
        has_next = jnp.where(s < n_sp - 1, 1, 0)
        r = iota(z.shape, 0)
        keep = jnp.where(r == 0, has_next, jnp.where(r < HALO, has_prev, 1))
        z = jnp.where(keep > 0, z, 0.0)
        taps = taps_ref[...].astype(F32)
        u = (
            taps[0:1] * pltpu.roll(z, 2, 0)
            + taps[1:2] * pltpu.roll(z, 1, 0)
            + taps[2:3] * z
            + taps[3:4] * pltpu.roll(z, total_rows - 1, 0)
        )
        return silu(u[HALO:])

    lane_row = iota((1, LANES), 1)
    expander = (
        iota((LANES, 2 * head_cols), 0) == iota((LANES, 2 * head_cols), 1) // HEAD_DIM
    ).astype(F32).astype(BF16)

    def expand(v):
        hi, lo = split(v)
        return dot(hi, expander) + dot(lo, expander)

    def decay_run(log_decay):
        size = log_decay.shape[0]
        i = iota((size, size), 0)
        j = iota((size, size), 1)
        pre = jnp.dot((j <= i).astype(F32), log_decay, precision=HIGHEST,
                      preferred_element_type=F32)
        total = pre[size - 1:size]
        suf = total - pre + log_decay
        return jnp.where(lane_row < heads, pre, suf), total

    blocks = [(d, g, (d * groups + g) % n_sp) for d in range(2) for g in range(groups)]

    def summarize(held, xs, bm, dt, run, total):
        weight = expand(jnp.exp(total - run) * dt)
        thi, tlo = split(jnp.broadcast_to(total, (16, LANES)))
        tail = jnp.where(
            iota((16, 2 * head_cols), 0) == 0, dot(thi, expander), dot(tlo, expander)
        ).astype(BF16)
        states = [
            dot_tn(bm, (xs * weight[:, d * head_cols:(d + 1) * head_cols]).astype(BF16))
            for d in range(2)
        ]
        for b, (d, g, _) in enumerate(blocks):
            lo = g * repeat_cols
            held[b, s, 0:STATE, :] = states[d][
                g * STATE:(g + 1) * STATE, lo:lo + repeat_cols
            ].astype(BF16)
            lo = d * head_cols + lo
            held[b, s, STATE:, :] = tail[:, lo:lo + repeat_cols]

    def to_owner(held, b, source, ssem, rsem):
        return remote(held.at[b, source], held.at[b, source], ssem.at[b],
                      rsem.at[b * n_sp + source], {"sp": blocks[b][2], "tp": t})

    def send_blocks(held, ssem, rsem):
        for b, (_, _, owner) in enumerate(blocks):
            pl.when(s != owner)(to_owner(held, b, s, ssem, rsem).start)

    hid_c[...] = (
        ctx_vals * ctx_rs * gain_row * (1.0 + scale[1:2]) + shift[1:2]
    ).astype(BF16)
    for i in (5, 6, 8, 9):
        loads[i].wait()
    ctx_x = conv(dot(hid_c[...], wx[...]), cx)
    ctx_b = conv(dot(hid_c[...], wb[...]), cb).astype(BF16)
    ctx_dt = softplus(dot_nt(hid_c[HALO:, :], wdt_all[...]))
    ctx_run, ctx_total = decay_run(rate_row * ctx_dt)
    summarize(ctx_st, ctx_x, ctx_b, ctx_dt, ctx_run, ctx_total)
    send_blocks(ctx_st, cm_send, cm_recv)

    for c in tok:
        c.wait_recv()
    low[0].wait_recv()
    high[0].wait_recv()
    lat_vals, lat_rs = normed_rows(lat_prev, lat_next, lat)
    hid_l[...] = (
        lat_vals * lat_rs * gain_row * (1.0 + scale[0:1]) + shift[0:1]
    ).astype(BF16)
    lat_x = conv(dot(hid_l[...], wx[...]), cx)
    lat_b = conv(dot(hid_l[...], wb[...]), cb).astype(BF16)
    dt = softplus(dot_nt(hid_l[HALO:, :], wdt_all[...]))
    run, total = decay_run(rate_row * dt + extra_all)
    summarize(lat_st, lat_x, lat_b, dt, run, total)
    send_blocks(lat_st, lm_send, lm_recv)

    loads[11].wait()
    loads[12].wait()
    lat_c = conv(dot(hid_l[...], wc[...]), cc).astype(BF16)
    run_t = jnp.transpose(run)
    dt_t = jnp.transpose(dt)
    i_pos = iota((length, length), 0)
    j_pos = iota((length, length), 1)
    lat_xb = lat_x.astype(BF16)
    state_lane = iota((length, state_cols), 1) // STATE
    pair_lane = iota((length, LANES), 1)
    zero_b = jnp.zeros((), BF16)
    per_group = heads // groups
    affinity = [
        dot_nt(jnp.where(state_lane == g, lat_c, zero_b), lat_b) for g in range(groups)
    ]

    def block_weights(h):
        ahead = heads + h
        gap = jnp.where(
            j_pos <= i_pos,
            run[:, h:h + 1] - run_t[h:h + 1, :],
            run[:, ahead:ahead + 1] - run_t[ahead:ahead + 1, :],
        )
        step = jnp.where(j_pos <= i_pos, dt_t[h:h + 1, :], 0.0) + jnp.where(
            j_pos >= i_pos, dt_t[ahead:ahead + 1, :], 0.0
        )
        return (affinity[h // per_group] * jnp.exp(gap) * step).astype(BF16)

    for q in range(heads // 2):
        both = lat_xb[:, q * LANES:(q + 1) * LANES]
        y_loc[:, q * LANES:(q + 1) * LANES] = dot(
            jnp.concatenate([block_weights(2 * q), block_weights(2 * q + 1)], axis=1),
            jnp.concatenate(
                [
                    jnp.where(pair_lane < HEAD_DIM, both, zero_b),
                    jnp.where(pair_lane >= HEAD_DIM, both, zero_b),
                ],
                axis=0,
            ),
        )
    reach = expand(jnp.exp(run))
    loads[13].wait()
    loads[14].wait()
    gate_act = silu(dot(hid_l[HALO:, :], wg[...]))

    def entry_copy(b, k):
        return remote(ent_tx.at[b, k], ent_rx.at[b], em_send.at[b * n_sp + k], em_recv.at[b],
                      {"sp": k, "tp": t})

    def growth(held, b, k):
        tail = held[b, k, STATE:, :].astype(F32)
        return jnp.exp(tail[0:1] + tail[1:2])

    def scan_block(b, d, owner):
        order = list(range(n_sp)) if d == 0 else list(range(n_sp - 1, -1, -1))
        for k in range(n_sp):
            if k != owner:
                to_owner(ctx_st, b, k, cm_send, cm_recv).wait_recv()
        state = jnp.zeros((STATE, repeat_cols), F32)
        for k in order:
            state = growth(ctx_st, b, k) * state + ctx_st[b, k, 0:STATE, :].astype(F32)
        for k in range(n_sp):
            if k != owner:
                to_owner(lat_st, b, k, lm_send, lm_recv).wait_recv()
        for k in order:
            entry = state.astype(BF16)
            if k == owner:
                ent_rx[b] = entry
            else:
                ent_tx[b, k] = entry
                entry_copy(b, k).start()
            state = growth(lat_st, b, k) * state + lat_st[b, k, 0:STATE, :].astype(F32)

    for b, (d, g, owner) in enumerate(blocks):
        pl.when(s == owner)(functools.partial(scan_block, b, d, owner))
    for b, (d, g, owner) in enumerate(blocks):
        pl.when(s != owner)(entry_copy(b, s).wait_recv)
    mixed_y = y_loc[...]
    zero_block = jnp.zeros((STATE, repeat_cols), BF16)
    for d in range(2):
        entry_all = jnp.concatenate(
            [
                jnp.concatenate(
                    [ent_rx[d * groups + g] if k == g else zero_block for k in range(groups)],
                    axis=1,
                )
                for g in range(groups)
            ],
            axis=0,
        )
        mixed_y = mixed_y + reach[:, d * head_cols:(d + 1) * head_cols] * dot(lat_c, entry_all)
    gated = mixed_y * gate_act
    og_row = flat_row(og[...].astype(F32))
    for g in range(groups):
        part_g = gated[:, g * repeat_cols:(g + 1) * repeat_cols]
        ms = jnp.mean(part_g * part_g, axis=-1, keepdims=True)
        nrm[:, g * repeat_cols:(g + 1) * repeat_cols] = (
            part_g * lax.rsqrt(ms + GROUP_EPS) * og_row[:, g * repeat_cols:(g + 1) * repeat_cols]
        ).astype(BF16)

    nm = []
    for d in range(1, n_tp):
        u = lax.rem(t + d, n_tp)
        c = remote(nrm.at[pl.ds(pl.multiple_of(u * rows, 16), rows)], nrm_rx.at[d],
                   nm_send.at[d], nm_recv.at[d], {"sp": s, "tp": u})
        c.start()
        nm.append(c)
    loads[15].wait()

    def out_rows(u):
        return wout[pl.ds(pl.multiple_of(u * head_cols, 16), head_cols), :]

    branch = dot(nrm[own_rows, :], out_rows(t))
    for d in range(1, n_tp):
        nm[d - 1].wait_recv()
        branch = branch + dot(nrm_rx[d], out_rows(lax.rem(t + n_tp - d, n_tp)))
    out_v[...] = (lat[own_rows, :].astype(F32) + gate_row * branch).astype(BF16)
    final = pltpu.make_async_copy(out_v, out_h, out_sem)
    final.start()

    for c in tok + ctx_halo + nm:
        c.wait_send()

    def sent(b, owner):
        to_owner(ctx_st, b, s, cm_send, cm_recv).wait_send()
        to_owner(lat_st, b, s, lm_send, lm_recv).wait_send()

    def handed(b, owner):
        for k in range(n_sp):
            if k != owner:
                entry_copy(b, k).wait_send()

    for b, (d, g, owner) in enumerate(blocks):
        pl.when(s != owner)(functools.partial(sent, b, owner))
        pl.when(s == owner)(functools.partial(handed, b, owner))

    @pl.when(t == n_tp - 1)
    def _():
        for c in low:
            c.wait_send()

    @pl.when(t == 0)
    def _():
        for c in high:
            c.wait_send()

    for d in range(1, n):
        other = lax.rem(rank + d, n)
        guarded(full, other < reducers, rs[d - 1].wait_send)

    def ag_done():
        for c in ag:
            c.wait_send()

    guarded(full, rank < reducers, ag_done)
    final.wait()


def local(
    latent, cond, context, context_cond, modulation, norm_gain, w_x, w_gate, w_b, w_c, w_dt,
    conv_x, conv_b, conv_c, decay_rate, decay_extra, out_gain, w_out,
):
    n_sp = lax.axis_size("sp")
    n_tp = lax.axis_size("tp")
    n = n_sp * n_tp
    rows, width = latent.shape
    length = decay_extra.shape[0]
    ctx_len = context.shape[0]
    mod_cols = modulation.shape[1]
    head_cols = w_x.shape[1]
    state_cols = w_b.shape[1]
    groups = state_cols // STATE
    repeat_cols = head_cols // groups
    reducers = max(m for m in range(1, n + 1) if mod_cols % (LANES * m) == 0)
    chunk = mod_cols // reducers

    args = (
        cond.reshape(-1, LANES), latent, context, modulation, norm_gain.reshape(-1, LANES),
        w_x, w_gate, w_b, w_c, jnp.swapaxes(w_dt, 1, 2), conv_x, conv_b, conv_c,
        decay_extra.T, out_gain.reshape(-1, LANES), w_out, context_cond.reshape(-1, LANES),
        decay_rate,
    )
    V = pltpu.VMEM
    D = pltpu.SemaphoreType.DMA
    held = [args[i] for i in (0, 3, 4, 5, 6, 7, 8, 9, 10, 11, 12, 13, 14, 15, 16, 17)]
    count = 2 * groups
    scratch = [V(a.shape, a.dtype) for a in held] + [
        V((2, width // LANES, LANES), F32),
        V((LANES, width), BF16),
        V((length, width), BF16),
        V((ctx_len, width), BF16),
        V((HALO, width), BF16),
        V((HALO, width), BF16),
        V((HALO, width), BF16),
        V((HALO, width), BF16),
        V((reducers, 2, chunk), F32),
        V((n, 2, chunk), F32),
        V((reducers, 2, chunk), F32),
        V((length + HALO, width), BF16),
        V((ctx_len + HALO, width), BF16),
        V((count, n_sp, STATE + 16, repeat_cols), BF16),
        V((count, n_sp, STATE + 16, repeat_cols), BF16),
        V((count, n_sp, STATE, repeat_cols), BF16),
        V((count, STATE, repeat_cols), BF16),
        V((length, head_cols), F32),
        V((length, head_cols), BF16),
        V((n_tp, rows, head_cols), BF16),
        V((rows, width), BF16),
        D((len(args),)),
        D((4 + 2 * n_tp,)),
        D((4,)),
        D((n_tp,)), D((n_tp,)),
        D((n,)), D((n,)), D((n,)), D((n,)),
        D((count,)), D((count * n_sp,)), D((count,)), D((count * n_sp,)),
        D((count * n_sp,)), D((count,)),
        D((n_tp,)), D((n_tp,)),
        D,
    ]
    return pl.pallas_call(
        functools.partial(mixer_kernel, n_sp, n_tp, reducers),
        out_shape=jax.ShapeDtypeStruct((rows, width), BF16),
        in_specs=[pl.BlockSpec(memory_space=pl.ANY)] * len(args),
        out_specs=pl.BlockSpec(memory_space=pl.ANY),
        scratch_shapes=scratch,
        compiler_params=pltpu.CompilerParams(
            collective_id=0, has_side_effects=True, vmem_limit_bytes=60 * 1024 * 1024
        ),
    )(*args)


def solution(mesh):
    in_specs = (
        P(("dp", "sp", "tp"), None),
        P("dp"),
        P(("dp", "sp"), None),
        P(),
        P(("sp", "tp"), None),
        P(),
        P(None, "tp"),
        P(None, "tp"),
        P(None, "tp"),
        P(None, "tp"),
        P(None, None, "tp"),
        P(None, "tp"),
        P(None, "tp"),
        P(None, "tp"),
        P(None, "tp"),
        P(("dp", "sp"), "tp"),
        P("tp"),
        P(),
    )
    out_specs = P(("dp", "sp", "tp"), None)
    return jax.shard_map(local, mesh=mesh, in_specs=in_specs, out_specs=out_specs, check_vma=False)
```
